32 devices in a mesh: fs: 8 (over z, x), tp: 4 (over y, core).
Axes of the slice: x: 2, y: 2, z: 4, core: 2. Of those that a mesh axis runs over, the one named last changes fastest.
Arguments:
- tokens: bfloat16 [3072, 4096], P('fs', 'tp'), may hold values from -600 to 600
- gate_master: float32 [8, 4096, 512], P(None, 'fs', 'tp'), may hold values from -0.09375 to 0.09375
- up_master: float32 [8, 4096, 512], P(None, 'fs', 'tp'), may hold values from -0.09375 to 0.09375
- down_master: float32 [8, 4096, 512], P(None, 'fs', 'tp'), may hold values from -0.25 to 0.25
- norm_gain: float32 [4096], P('fs'), may hold values from 0.1 to 1.9
- routes: int32 [3072, 2], P('fs'), may hold values from 0 to 7, all different within a row; in each aligned block of 384 rows (0 to 383, 384 to 767, ...) at most 192 rows name the same one
- route_weight: float32 [3072, 2], P('fs'), may hold values from 0.1 to 1
Outputs:
- gate_out: bfloat16 [8, 4096, 512], P('fs', None, 'tp')
- up_out: bfloat16 [8, 4096, 512], P('fs', None, 'tp')
- down_out: bfloat16 [8, 4096, 512], P('fs', None, 'tp')
- mixed: bfloat16 [3072, 4096], P('fs', 'tp')
The draws below stay inside these ranges and needn't reach their ends.
Inputs may be any that keep to these rules, and one draw needn't show every extreme that they name: `routes`: within the rows of one index of fs no expert is named by more than 192 pairs, a bound that some block reaches; the 2 experts of a row differ.
All inputs are finite; a program needn't handle non-finite values.
Results may differ from the reference program's by a relative error of at most 0.0087.
Values may be sent and summed in bfloat16 or wider, within the bound.
A program may use at most 128 MiB of HBM per device.

```python
import math
import jax
import jax.numpy as jnp
import numpy as np
from jax import lax

D = 4096
FF = 512
TOP = 2
TOK_DEV = 384
EXPERTS = 8
TOKENS = 3072
CAP = 192
N_FS = 8


def draw_tokens(key, part):
    k_base, k_rows, k_cols = jax.random.split(key, 3)
    row_scale = jnp.exp(jax.random.uniform(k_rows, (TOKENS, 1), jnp.float32) * math.log(10.0))
    position = jnp.arange(D, dtype=jnp.float32)[None, :] / D
    col_scale = jnp.exp(position * math.log(3.0) + jax.random.uniform(k_cols, (1, D), jnp.float32) * math.log(3.3))
    base = jnp.clip(jax.random.normal(k_base, (TOKENS, D), jnp.float32), -6.0, 6.0)
    return (base * row_scale * col_scale).astype(jnp.bfloat16)


def shard_levels(own_key, extent, cuts, low, high):
    def one(dim, shards_of):
        steps = jax.random.uniform(jax.random.fold_in(jax.random.fold_in(own_key, 6), dim), (shards_of,), jnp.float32, low / len(cuts), high / len(cuts))
        return jnp.repeat(jnp.exp(steps), extent[dim] // shards_of).reshape((-1,) + (1,) * (len(extent) - dim - 1))

    factor_of = one(*cuts[0])
    for cut in cuts[1:]:
        factor_of = factor_of * one(*cut)
    return factor_of


def assign_block(own_key, own, number, rows, amount, top, most, slope):
    ranking = jax.random.permutation(own_key, amount)
    packed, ordinary = load_shares(amount, rows * top, most, slope, True), load_shares(amount, rows * top, most, slope, False)
    places = jnp.arange(amount)

    def named(sizes, rotation):
        used = int((sizes > 0).sum())
        fixed = max(1, used // 4)
        passed = fixed + (places - fixed + rotation * (used - fixed)) % max(1, amount - fixed)
        return jnp.zeros((amount,), jnp.int32).at[ranking[jnp.where(places < fixed, places, passed)]].set(jnp.asarray(sizes, jnp.int32))

    sizes = jnp.where(number % 4 == 0, named(packed, number // 4), named(ordinary, number - number // 4 - 1))
    mixed = jax.random.permutation(jax.random.fold_in(own, 3), amount)
    giver, taker = mixed[0:amount // 2 * 2:2], mixed[1:amount // 2 * 2:2]
    room = jnp.minimum(sizes[giver] - 1, most - sizes[taker]) // 2
    room = jnp.where((giver == ranking[0]) | (taker == ranking[0]) | (sizes[taker] == 0), 0, jnp.maximum(room, 0))
    passed = jax.random.randint(jax.random.fold_in(own, 4), (amount // 2,), 0, 1 << 20) % (room + 1)
    sizes = sizes.at[giver].add(-passed).at[taker].add(passed)
    members = jnp.searchsorted(jnp.cumsum(sizes), jnp.arange(rows * top), side="right").astype(jnp.int32)
    grid = members.reshape(top, rows).T
    grid = grid[jax.random.permutation(jax.random.fold_in(own, 1), rows)]
    rotation = jax.random.randint(jax.random.fold_in(own, 2), (rows, 1), 0, top)
    return jnp.take_along_axis(grid, (jnp.arange(top)[None, :] + rotation) % top, axis=1)


def load_shares(number_of, total, reach, skew, full):
    portions = [(1 << 20) // math.isqrt(rank ** skew) + 1 for rank in range(1, number_of + 1)]
    largest = reach if full else min(reach, max(-(-total // number_of), total * portions[0] // sum(portions)))
    least = 1 if total - largest >= number_of - 1 else 0
    holding, surplus = [largest] + [least] * (number_of - 1), total - largest - least * (number_of - 1)
    while surplus > 0:
        free = [i for i in range(1, number_of) if holding[i] < largest] or [i for i in range(1, number_of) if holding[i] < reach]
        pool, remaining = sum([portions[i] for i in free]), surplus
        for i in free:
            addition = min(reach - holding[i], max(1, remaining * portions[i] // pool), surplus)
            holding[i] = holding[i] + addition
            surplus = surplus - addition
    return np.array(holding)


def bell_draw(key, extent, width, bound, shards=(), kind=jnp.bfloat16):
    values = jax.random.normal(key, extent, jnp.float32) * width
    if len(shards) > 0:
        values = shard_levels(key, extent, shards, -0.22, 0.18) * values
    return jnp.clip(values, min=-bound, max=bound).astype(kind)


def setup_inputs(seed: int = 0) -> dict:
    keys = jax.random.split(jax.random.key(seed), 8)
    tokens = draw_tokens(jax.random.fold_in(keys[7], 71), 0)
    gate_master = bell_draw(keys[1], (EXPERTS, D, FF), D ** -0.5, 0.09375, ((1, 8), (2, 4)), jnp.float32)
    up_master = bell_draw(keys[2], (EXPERTS, D, FF), D ** -0.5, 0.09375, ((1, 8), (2, 4)), jnp.float32)
    down_master = bell_draw(keys[3], (EXPERTS, D, FF), FF ** -0.5, 0.25, ((1, 8), (2, 4)), jnp.float32)
    norm_gain = jnp.clip(1.0 + 0.18 * jax.random.normal(keys[4], (D,), jnp.float32), 0.1, 1.9)
    routes_keys = jax.random.split(jax.random.fold_in(keys[5], 1), TOKENS // TOK_DEV)
    routes_turns = jax.random.permutation(jax.random.fold_in(keys[5], 3), TOKENS // TOK_DEV)
    routes = jax.vmap(lambda own, number: assign_block(jax.random.fold_in(keys[5], 2), own, number, TOK_DEV, EXPERTS, TOP, CAP, 2))(routes_keys, routes_turns).reshape((TOKENS, TOP))
    route_weight = jnp.clip(jnp.exp(math.log(1.0) - 2.3025851 * jax.random.uniform(keys[6], (TOKENS, TOP), jnp.float32) ** shard_levels(keys[6], (TOKENS, TOP), ((0, 8),), -0.2, 0.2)), 0.1, 1.0)
    return dict(tokens=tokens, gate_master=gate_master, up_master=up_master, down_master=down_master, norm_gain=norm_gain, routes=routes, route_weight=route_weight)


norm_eps = 1e-06

def slot_table(expert_ids, n_experts, capacity, top_count):
    assigned = expert_ids.shape[0]
    onehot = (expert_ids[:, None] == jnp.arange(n_experts, dtype=jnp.int32)[None, :]).astype(jnp.int32)
    before = jnp.cumsum(onehot, axis=0) - onehot
    slots = lax.optimization_barrier(jnp.sum(before * onehot, axis=1)).astype(jnp.int32)
    position = expert_ids * capacity + slots
    owners = jnp.arange(assigned, dtype=jnp.int32) // top_count
    matches = position[None, :] == jnp.arange(n_experts * capacity, dtype=jnp.int32)[:, None]
    slot_token = lax.optimization_barrier(jnp.max(jnp.where(matches, owners[None, :], -1), axis=1)).astype(jnp.int32)
    return (slots, slot_token)

def reference(tokens, gate_master, up_master, down_master, norm_gain, routes, route_weight):
    folded = norm_gain[None, :, None]
    gate_out = (gate_master * folded).astype(jnp.bfloat16)
    up_out = (up_master * folded).astype(jnp.bfloat16)
    down_out = down_master.astype(jnp.bfloat16)
    token_float = tokens.astype(jnp.float32)
    inverse = lax.rsqrt(lax.optimization_barrier(jnp.mean(token_float * token_float, axis=1, keepdims=True)) + norm_eps)
    normed = (token_float * inverse).astype(jnp.bfloat16)
    mix_weights = route_weight / lax.optimization_barrier(jnp.sum(route_weight, axis=1, keepdims=True))
    block_routes = routes.reshape(N_FS, TOK_DEV * TOP)

    def per_block(one_block):
        return slot_table(one_block, EXPERTS, CAP, TOP)
    slots, slot_token = jax.vmap(per_block)(block_routes)
    offsets = jnp.arange(N_FS, dtype=jnp.int32)[:, None] * TOK_DEV
    global_token = jnp.where(slot_token < 0, TOKENS, slot_token + offsets).astype(jnp.int32)
    padded = jnp.concatenate([normed, jnp.zeros((1, D), jnp.bfloat16)], axis=0)

    def run_expert(expert):
        columns = lax.dynamic_slice_in_dim(global_token, expert * CAP, CAP, 1).reshape(-1)
        expert_rows = padded[columns]
        gate_mat = lax.dynamic_index_in_dim(gate_out, expert, 0, keepdims=False)
        up_mat = lax.dynamic_index_in_dim(up_out, expert, 0, keepdims=False)
        down_mat = lax.dynamic_index_in_dim(down_out, expert, 0, keepdims=False)
        gate_val = jnp.dot(expert_rows, gate_mat, preferred_element_type=jnp.float32)
        up_val = jnp.dot(expert_rows, up_mat, preferred_element_type=jnp.float32)
        hidden = (jax.nn.silu(gate_val) * up_val).astype(jnp.bfloat16)
        result = lax.dot_general(hidden, down_mat, (((1,), (1,)), ((), ())), preferred_element_type=jnp.float32)
        return result.astype(jnp.bfloat16)
    outputs = lax.map(run_expert, jnp.arange(EXPERTS, dtype=jnp.int32))
    flat_out = outputs.reshape(-1, D)
    block_index = jnp.arange(N_FS, dtype=jnp.int32)[:, None]
    index = ((block_routes * N_FS + block_index) * CAP + slots).astype(jnp.int32)
    gathered = flat_out[index.reshape(-1)].astype(jnp.float32).reshape(TOKENS, TOP, D)
    mixed = lax.optimization_barrier(jnp.sum(mix_weights[:, :, None] * gathered, axis=1)).astype(jnp.bfloat16)
    return (gate_out, up_out, down_out, mixed)
```

```python
import functools

import jax
import jax.numpy as jnp
from jax import lax
from jax.experimental import pallas as pl
from jax.experimental.pallas import tpu as pltpu
from jax.sharding import PartitionSpec as P

norm_eps = 1e-06


def half_shift(step, size):
    half = size // 2
    return [(s, s // half * half + (s % half + step) % half) for s in range(size)]


def cross_swap(size):
    return [(s, (s + size // 2) % size) for s in range(size)]


def member_shift(step, crossed, size):
    half = size // 2
    return [
        (s, (s // half + crossed) % 2 * half + (s % half + step) % half) for s in range(size)
    ]


def plain_body(tokens, gate_master, up_master, down_master, norm_gain, routes, route_weight):
    n_experts = gate_master.shape[0]
    tok_rows, top_count = routes.shape
    capacity = 2 * tok_rows * top_count // n_experts
    n_tp = lax.axis_size("tp")
    half = n_tp // 2
    width = tokens.shape[1]
    hidden_cols = gate_master.shape[2]
    me_tp = lax.axis_index("tp")
    chunks = 2 if capacity % 32 == 0 else 1
    part = capacity // chunks

    folded = norm_gain[None, :, None]
    trio = jnp.concatenate(
        [
            (gate_master * folded).astype(jnp.bfloat16),
            (up_master * folded).astype(jnp.bfloat16),
            down_master.astype(jnp.bfloat16),
        ],
        axis=2,
    )
    trio = lax.all_to_all(trio, "fs", split_axis=0, concat_axis=1, tiled=True)
    pair = trio[:, :, : 2 * hidden_cols]
    gate_out = trio[:, :, :hidden_cols]
    up_out = trio[:, :, hidden_cols : 2 * hidden_cols]
    down_out = trio[:, :, 2 * hidden_cols :]

    token_float = tokens.astype(jnp.float32)
    sumsquares = lax.psum(jnp.sum(token_float * token_float, axis=1), "tp")
    inverse = lax.rsqrt(sumsquares / (width * n_tp) + norm_eps)[:, None]
    normed = (token_float * inverse).astype(jnp.bfloat16)
    mix = route_weight / jnp.sum(route_weight, axis=1, keepdims=True)
    experts = jnp.arange(n_experts, dtype=jnp.int32)
    named = jnp.any(routes[:, :, None] == experts, axis=1)
    earlier = jnp.arange(tok_rows)[:, None] > jnp.arange(tok_rows)[None, :]
    before = jnp.dot(
        earlier.astype(jnp.bfloat16), named.astype(jnp.bfloat16), preferred_element_type=jnp.float32
    ).astype(jnp.int32)
    slots = jnp.sum(jnp.where(routes[:, :, None] == experts, before[:, None, :], 0), axis=2)
    place = (slots // part * n_experts + routes) * part + slots % part
    spots = jnp.arange(n_experts * capacity, dtype=jnp.int32)
    where_to = place[:, :, None] == spots
    onehot = jnp.any(where_to, axis=1).astype(jnp.bfloat16)
    mixing = jnp.sum(jnp.where(where_to, mix[:, :, None], 0.0), axis=1)
    mixing = mixing.astype(jnp.bfloat16)
    outgoing = lax.dot_general(
        onehot, normed, (((0,), (0,)), ((), ())), preferred_element_type=jnp.float32
    ).astype(jnp.bfloat16)
    outgoing = outgoing.reshape(chunks, n_experts, part, width)

    my_half = me_tp // half
    inside = me_tp % half
    span = half * width
    own_cols = lax.dynamic_slice_in_dim(pair[0], my_half * span, span, 0)
    partner_cols = lax.ppermute(
        lax.dynamic_slice_in_dim(pair[0], (1 - my_half) * span, span, 0), "tp", cross_swap(n_tp)
    )

    arrived = []
    for c in range(chunks):
        if c == 0:
            ready, trio = lax.optimization_barrier((outgoing[c], trio))
        else:
            ready, arrived[-1], partner_cols = lax.optimization_barrier((outgoing[c], last, partner_cols))
        last = lax.all_to_all(ready, "fs", split_axis=0, concat_axis=0, tiled=True)
        arrived.append(last)

    def in_order(cols):
        blocks = cols.reshape(half, width, cols.shape[1])
        return [
            lax.dynamic_index_in_dim(blocks, (inside + half - j) % half, 0, keepdims=False)
            for j in range(half)
        ]

    own_blocks, partner_blocks = in_order(own_cols), in_order(partner_cols)
    quarters = down_out[0].reshape(n_tp, -1, hidden_cols)
    picked = []
    for j in range(half):
        for crossed in range(2):
            target = (my_half + crossed) % 2 * half + (inside + j) % half
            piece = lax.dynamic_index_in_dim(quarters, target, 0, keepdims=False)
            if j + crossed > 0:
                piece = lax.ppermute(piece, "tp", member_shift(j, crossed, n_tp))
            picked.append(piece)
    down_mat = jnp.concatenate(picked, axis=1)

    def serve(rows):
        rows = rows.reshape(-1, width)
        pieces = [rows] + [lax.ppermute(rows, "tp", half_shift(j, n_tp)) for j in range(1, half)]

        def partial(blocks):
            total = 0.0
            for piece, block in zip(pieces, blocks):
                total = total + jnp.dot(piece, block, preferred_element_type=jnp.float32)
            return total

        swapped = lax.ppermute(partial(partner_blocks).astype(jnp.bfloat16), "tp", cross_swap(n_tp))
        both = partial(own_blocks) + swapped.astype(jnp.float32)
        hidden = (jax.nn.silu(both[:, :hidden_cols]) * both[:, hidden_cols:]).astype(jnp.bfloat16)
        two = jnp.concatenate([hidden, lax.ppermute(hidden, "tp", cross_swap(n_tp))], axis=1)
        all_hidden = [two] + [lax.ppermute(two, "tp", half_shift(j, n_tp)) for j in range(1, half)]
        result = lax.dot_general(
            jnp.concatenate(all_hidden, axis=1),
            down_mat,
            (((1,), (1,)), ((), ())),
            preferred_element_type=jnp.float32,
        )
        return result.astype(jnp.bfloat16).reshape(-1, part, width)

    returned = []
    for c in range(chunks):
        rows = arrived[c]
        if c > 0:
            rows, served = lax.optimization_barrier((rows, served))
            returned.append(lax.all_to_all(served, "fs", split_axis=0, concat_axis=0, tiled=True))
        served = serve(rows)
    returned.append(lax.all_to_all(served, "fs", split_axis=0, concat_axis=0, tiled=True))

    mixed = 0.0
    for c, back in enumerate(returned):
        flat = back.reshape(n_experts * part, width)
        chosen = mixing[:, c * n_experts * part : (c + 1) * n_experts * part]
        mixed = mixed + jnp.dot(chosen, flat, preferred_element_type=jnp.float32)
    return (gate_out, up_out, down_out, mixed.astype(jnp.bfloat16))


PAIR = 2
VMEM_BUDGET = 62 * 1024 * 1024


def near_first(n_z):
    return [sorted(range(n_z), key=lambda b: (abs(b - z), b)) for z in range(n_z)]


def far_first(n_z):
    def rank(z, b):
        return (-abs(b - z), min(b, n_z - 1 - b), b)

    return [sorted(range(n_z), key=lambda b: rank(z, b)) for z in range(n_z)]


def looked_up(table, z, step):
    chosen = 0
    for i, row in enumerate(table):
        for s, value in enumerate(row):
            chosen = chosen + jnp.where((z == i) & (step == s), value, 0)
    return chosen


def moe_kernel(
    dims,
    tok, gain, routes, weight, gate_hbm, up_hbm, down_hbm,
    gate_out, up_out, down_out, mixed_out,
    stage, wgu_send, wd_send, wgu_recv, wd_recv, blk, rows, xsend, hid, dn, yb, ysend,
    rs_send, rs_recv, acc, ssq, aux_send, aux_recv, gain_mat,
    stage_sem, ssq_s, ssq_r, aux_s, aux_r, ag_sr, ag_sl, ag_r,
    wgu_s, wgu_r, wd_s, wd_r, x_s, x_r,
    rc_s, rc_r, ry_s, ry_r, rf_s, rf_r,
    hc_s, hc_r, hy_s, hy_r, hf_s, hf_r,
    dn_s, dn_r, y_s, y_r, rs_sr, rs_sl, rs_r, out_sem,
):
    n_fs, n_tp, n_z, r_rows, feat, d_loc, h_cols, cap = dims
    top_count = routes.shape[0]
    f32, bf16 = jnp.float32, jnp.bfloat16
    me = lax.axis_index("fs")
    t = lax.axis_index("tp")
    z, x = me // PAIR, me % PAIR
    xp = me - x + (1 - x)
    half = n_tp // 2
    tc = (t // half) * half + (half - 1 - t % half)
    ty = (t + half) % n_tp
    near, far = near_first(n_z), far_first(n_z)
    per_quarter = feat // d_loc

    def remote(src, dst, ssem, rsem, **where):
        return pltpu.make_async_remote_copy(
            src_ref=src, dst_ref=dst, send_sem=ssem, recv_sem=rsem,
            device_id=where, device_id_type=pl.DeviceIdType.MESH,
        )

    masters = (gate_hbm, up_hbm, down_hbm)

    def load(i, e):
        return pltpu.make_async_copy(masters[i].at[e], stage.at[i, e], stage_sem.at[i, e])

    def every(count, body):
        def step(i, carry):
            body(i)
            return carry
        lax.fori_loop(0, count, step, 0)

    barrier = pltpu.get_barrier_semaphore()
    for d in range(1, n_fs):
        pl.semaphore_signal(barrier, inc=1, device_id={"fs": (me + d) % n_fs},
                            device_id_type=pl.DeviceIdType.MESH)
    for d in range(1, n_tp):
        pl.semaphore_signal(barrier, inc=1, device_id={"tp": (t + d) % n_tp},
                            device_id_type=pl.DeviceIdType.MESH)

    def start_load(d):
        for i in range(3):
            load(i, (me + d) % n_fs).start()
    every(n_fs, start_load)

    value = tok[...].astype(f32)
    column = jnp.sum(value * value, axis=1, keepdims=True)
    spread = jnp.transpose(jnp.broadcast_to(column, (r_rows, 128)))
    ssq[t] = spread[:8]

    pl.semaphore_wait(barrier, n_fs - 1 + n_tp - 1)

    def ssq_copy(d):
        peer = (t + d) % n_tp
        return remote(ssq.at[t], ssq.at[t], ssq_s.at[d], ssq_r.at[t], tp=peer)

    def ssq_from(d):
        peer = (t + n_tp - d) % n_tp
        return remote(ssq.at[peer], ssq.at[peer], ssq_s.at[d], ssq_r.at[peer], tp=peer)
    for d in range(1, n_tp):
        ssq_copy(d).start()

    expert = lax.broadcasted_iota(jnp.int32, (n_fs, r_rows), 0)
    picks = [jnp.broadcast_to(routes[k : k + 1, :], (n_fs, r_rows)) == expert for k in range(top_count)]
    weights = weight[...]
    mix = weights / jnp.sum(weights, axis=0, keepdims=True)
    named = jnp.zeros((n_fs, r_rows), f32)
    mixed_t = jnp.zeros((n_fs, r_rows), f32)
    for k in range(top_count):
        named = named + jnp.where(picks[k], 1.0, 0.0)
        mixed_t = mixed_t + jnp.where(picks[k], jnp.broadcast_to(mix[k : k + 1, :], (n_fs, r_rows)), 0.0)
    first = lax.broadcasted_iota(jnp.int32, (r_rows, r_rows), 0)
    second = lax.broadcasted_iota(jnp.int32, (r_rows, r_rows), 1)
    earlier = jnp.where(first < second, 1.0, 0.0).astype(bf16)
    before = jnp.dot(named.astype(bf16), earlier, preferred_element_type=f32)
    slot_t = jnp.where(named > 0.0, before, -1.0)
    for plane in range(n_z):
        lo = plane * PAIR
        aux_send[plane, 0:PAIR, :] = slot_t[lo : lo + PAIR]
        aux_send[plane, PAIR : 2 * PAIR, :] = mixed_t[lo : lo + PAIR]
        aux_send[plane, 2 * PAIR :, :] = jnp.zeros((8 - 2 * PAIR, r_rows), f32)
    aux_recv[z] = aux_send[z]

    def aux_copy(d):
        plane = (z + d) % n_z
        return remote(aux_send.at[plane], aux_recv.at[z], aux_s.at[d], aux_r.at[z], fs=plane * PAIR + x)

    def aux_from(plane):
        return remote(aux_send.at[plane], aux_recv.at[plane], aux_s.at[0], aux_r.at[plane], fs=me)
    for d in range(1, n_z):
        aux_copy(d).start()

    gain_mat[...] = jnp.transpose(jnp.broadcast_to(gain[...], (h_cols, d_loc)))

    def wgu_copy(d):
        e = (me + d) % n_fs
        return remote(wgu_send.at[e], wgu_recv.at[me], wgu_s.at[d], wgu_r.at[me], fs=e)

    def wgu_from(j):
        return remote(wgu_send.at[j], wgu_recv.at[j], wgu_s.at[0], wgu_r.at[j], fs=me)

    def wd_copy(d):
        e = (me + d) % n_fs
        return remote(wd_send.at[e], wd_recv.at[me], wd_s.at[d], wd_r.at[me], fs=e)

    def wd_from(j):
        return remote(wd_send.at[j], wd_recv.at[j], wd_s.at[0], wd_r.at[j], fs=me)

    def cast_gu(d, target, index):
        e = (me + d) % n_fs
        load(0, e).wait()
        load(1, e).wait()
        target[index, :, 0:h_cols] = (stage[0, e] * gain_mat[...]).astype(bf16)
        target[index, :, h_cols : 2 * h_cols] = (stage[1, e] * gain_mat[...]).astype(bf16)

    def cast_d(d, target, index):
        e = (me + d) % n_fs
        load(2, e).wait()
        target[index] = stage[2, e].astype(bf16)

    def send_gu(d):
        cast_gu(d, wgu_send, (me + d) % n_fs)
        wgu_copy(d).start()

    def send_d(d):
        cast_d(d, wd_send, (me + d) % n_fs)
        wd_copy(d).start()

    def span(first_d, last_d, body):
        every(last_d - first_d, lambda i: body(i + first_d))

    for d in range(1, n_tp):
        ssq_from(d).wait_recv()
    total = ssq[0]
    for k in range(1, n_tp):
        total = total + ssq[k]
    inverse = lax.rsqrt(total / (feat * n_tp) + norm_eps)
    inverse = jnp.transpose(jnp.broadcast_to(inverse[0:1], (128, r_rows)))[:, 0:1]
    blk[z] = (tok[...].astype(f32) * inverse).astype(bf16)

    def ag_right(b):
        return remote(blk.at[b], blk.at[b], ag_sr.at[b], ag_r.at[b], fs=me + PAIR)

    def ag_left(b):
        return remote(blk.at[b], blk.at[b], ag_sl.at[b], ag_r.at[b], fs=me - PAIR)

    def goes_right(b):
        return (b <= z) & (z < n_z - 1)

    def goes_left(b):
        return (b >= z) & (z > 0)

    def picker(b, which):
        slots = aux_recv[b, pl.ds(which, 1), :]
        at = lax.broadcasted_iota(jnp.int32, (cap, r_rows), 0).astype(f32)
        return at == jnp.broadcast_to(slots, (cap, r_rows))

    def x_copy(b):
        return remote(xsend.at[b], rows.at[t, b, pl.ds(cap, cap)], x_s.at[b], x_r.at[b], fs=xp)

    def stage_a(s):
        b = looked_up(near, z, s)

        @pl.when(b != z)
        def _():
            ag_right(b).wait_recv()
            aux_from(b).wait_recv()

        @pl.when(goes_right(b))
        def _():
            ag_right(b).start()

        @pl.when(goes_left(b))
        def _():
            ag_left(b).start()
        theirs = jnp.where(picker(b, 1 - x), 1.0, 0.0).astype(bf16)
        xsend[b] = jnp.dot(theirs, blk[b], preferred_element_type=f32).astype(bf16)
        x_copy(b).start()
        ours = jnp.where(picker(b, x), 1.0, 0.0).astype(bf16)
        rows[t, b, 0:cap, :] = jnp.dot(ours, blk[b], preferred_element_type=f32).astype(bf16)

    def rc_copy(b):
        return remote(rows.at[t, b], rows.at[t, b], rc_s.at[b], rc_r.at[b], tp=tc)

    def ry_copy(b):
        return remote(rows.at[t, b], rows.at[t, b], ry_s.at[b], ry_r.at[b], tp=ty)

    def rf_copy(b):
        return remote(rows.at[ty, b], rows.at[ty, b], rf_s.at[b], rf_r.at[b], tp=tc)

    def stage_b(s):
        b = looked_up(near, z, s)
        x_copy(b).wait_recv()
        ry_copy(b).start()
        rc_copy(b).start()

    def stage_c(s):
        b = looked_up(near, z, s)
        ry_copy(b).wait_recv()
        rf_copy(b).start()

    stage_a(0)
    span(1, 3, send_gu)
    stage_b(0)
    span(3, 5, send_gu)
    stage_a(1)
    span(5, 7, send_gu)
    stage_c(0)
    stage_b(1)
    span(7, n_fs, send_gu)
    span(1, 3, send_d)
    stage_a(2)
    stage_c(1)
    stage_b(2)
    span(3, 5, send_d)
    stage_a(3)
    span(5, n_fs, send_d)
    stage_c(2)
    stage_b(3)
    cast_gu(0, wgu_recv, me)
    cast_d(0, wd_recv, me)
    stage_c(3)

    def wait_gu(d):
        wgu_from((me + n_fs - d) % n_fs).wait_recv()
    span(1, n_fs, wait_gu)

    def hc_copy(b):
        return remote(hid.at[t, b], hid.at[t, b], hc_s.at[b], hc_r.at[b], tp=tc)

    def hy_copy(b):
        return remote(hid.at[t, b], hid.at[t, b], hy_s.at[b], hy_r.at[b], tp=ty)

    def hf_copy(b):
        return remote(hid.at[ty, b], hid.at[ty, b], hf_s.at[b], hf_r.at[b], tp=tc)

    def stage_d(s):
        b = looked_up(far, z, s)
        rc_copy(b).wait_recv()
        rf_copy(b).wait_recv()
        both = jnp.zeros((2 * cap, 2 * h_cols), f32)
        for j in range(n_fs):
            lo = (j % per_quarter) * d_loc
            both = both + jnp.dot(rows[j // per_quarter, b, :, lo : lo + d_loc], wgu_recv[j],
                                  preferred_element_type=f32)
        gates = both[:, 0:h_cols]
        hid[t, b] = (gates / (1.0 + jnp.exp(-gates)) * both[:, h_cols:]).astype(bf16)
        hy_copy(b).start()
        hc_copy(b).start()
    every(n_z, stage_d)

    def out_copies(j):
        at = pl.ds(pl.multiple_of(j * d_loc, d_loc), d_loc)
        return [
            pltpu.make_async_copy(wgu_recv.at[j, :, pl.ds(0, h_cols)], gate_out.at[at], out_sem.at[0, j]),
            pltpu.make_async_copy(wgu_recv.at[j, :, pl.ds(h_cols, h_cols)], up_out.at[at], out_sem.at[1, j]),
            pltpu.make_async_copy(wd_recv.at[j], down_out.at[at], out_sem.at[2, j]),
        ]

    def dn_copy(j):
        q = j % per_quarter
        return remote(wd_recv.at[j], dn.at[q, t], dn_s.at[j], dn_r.at[q, t], tp=j // per_quarter)

    def dn_from(q, k):
        return remote(wd_recv.at[0], dn.at[q, k], dn_s.at[0], dn_r.at[q, k], tp=t)

    def pass_down(d):
        j = (me + n_fs - d) % n_fs

        @pl.when(d > 0)
        def _():
            wd_from(j).wait_recv()

        @pl.when(j // per_quarter == t)
        def _():
            dn[j % per_quarter, t] = wd_recv[j]

        @pl.when(j // per_quarter != t)
        def _():
            dn_copy(j).start()
        for copy in out_copies(j):
            copy.start()
    every(n_fs, pass_down)

    def stage_e(s):
        b = looked_up(far, z, s)
        hy_copy(b).wait_recv()
        hf_copy(b).start()
    every(n_z, stage_e)

    def wait_dn(d):
        k = (t + d) % n_tp
        for q in range(per_quarter):
            dn_from(q, k).wait_recv()
    span(1, n_tp, wait_dn)

    def y_copy(b):
        return remote(ysend.at[b], yb.at[b, pl.ds(cap, cap)], y_s.at[b], y_r.at[b], fs=xp)

    def stage_f(s):
        b = looked_up(far, z, s)
        hc_copy(b).wait_recv()
        hf_copy(b).wait_recv()
        units = jnp.concatenate([hid[k, b] for k in range(n_tp)], axis=1)
        for q in range(per_quarter):
            mat = jnp.concatenate([dn[q, k] for k in range(n_tp)], axis=1)
            result = lax.dot_general(units, mat, (((1,), (1,)), ((), ())), preferred_element_type=f32)
            result = result.astype(bf16)
            lo = q * d_loc
            ysend[b, :, lo : lo + d_loc] = result[cap:]
            yb[b, 0:cap, lo : lo + d_loc] = result[:cap]
        y_copy(b).start()
    every(n_z, stage_f)

    def rs_right(b):
        return remote(rs_send.at[b], rs_recv.at[b], rs_sr.at[b], rs_r.at[b], fs=me + PAIR)

    def rs_left(b):
        at = jnp.where(b == z - 1, n_z, b)
        return remote(rs_send.at[b], rs_recv.at[at], rs_sl.at[b], rs_r.at[at], fs=me - PAIR)

    def rs_from(at):
        return remote(rs_send.at[0], rs_recv.at[at], rs_sr.at[0], rs_r.at[at], fs=me)

    def stage_g(s):
        b = looked_up(far, z, s)
        y_copy(b).wait_recv()

        def share(which):
            weights = jnp.broadcast_to(aux_recv[b, pl.ds(PAIR + which, 1), :], (cap, r_rows))
            return jnp.where(picker(b, which), weights, 0.0).astype(bf16)
        spreading = jnp.concatenate([share(x), share(1 - x)], axis=0)
        acc[...] = lax.dot_general(spreading, yb[b], (((0,), (0,)), ((), ())), preferred_element_type=f32)

        @pl.when(((b >= z) & (z > 0)) | ((b < z) & (z < n_z - 1)))
        def _():
            rs_from(b).wait_recv()
            acc[...] += rs_recv[b].astype(f32)

        @pl.when((b == z) & (z < n_z - 1))
        def _():
            rs_from(n_z).wait_recv()
            acc[...] += rs_recv[n_z].astype(f32)

        @pl.when(b != z)
        def _():
            rs_send[b] = acc[...].astype(bf16)

        @pl.when(b > z)
        def _():
            rs_right(b).start()

        @pl.when(b < z)
        def _():
            rs_left(b).start()

        @pl.when(b == z)
        def _():
            mixed_out[...] = acc[...].astype(bf16)
    every(n_z, stage_g)

    for d in range(1, n_tp):
        ssq_copy(d).wait_send()
    for d in range(1, n_z):
        aux_copy(d).wait_send()

    def sent_w(d):
        wgu_copy(d).wait_send()
        wd_copy(d).wait_send()
    span(1, n_fs, sent_w)

    def sent_b(b):
        @pl.when(goes_right(b))
        def _():
            ag_right(b).wait_send()

        @pl.when(goes_left(b))
        def _():
            ag_left(b).wait_send()
        for copy in (x_copy, rc_copy, ry_copy, rf_copy, hc_copy, hy_copy, hf_copy, y_copy):
            copy(b).wait_send()

        @pl.when(b > z)
        def _():
            rs_right(b).wait_send()

        @pl.when(b < z)
        def _():
            rs_left(b).wait_send()
    every(n_z, sent_b)

    def sent_j(j):
        @pl.when(j // per_quarter != t)
        def _():
            dn_copy(j).wait_send()
        for copy in out_copies(j):
            copy.wait()
    every(n_fs, sent_j)


def scratch_for(dims):
    n_fs, n_tp, n_z, r_rows, feat, d_loc, h_cols, cap = dims
    f32, bf16 = jnp.float32, jnp.bfloat16
    per_quarter = feat // d_loc
    buffers = [
        ((3, n_fs, d_loc, h_cols), f32),
        ((n_fs, d_loc, 2 * h_cols), bf16),
        ((n_fs, d_loc, h_cols), bf16),
        ((n_fs, d_loc, 2 * h_cols), bf16),
        ((n_fs, d_loc, h_cols), bf16),
        ((n_z, r_rows, feat), bf16),
        ((n_tp, n_z, 2 * cap, feat), bf16),
        ((n_z, cap, feat), bf16),
        ((n_tp, n_z, 2 * cap, h_cols), bf16),
        ((per_quarter, n_tp, d_loc, h_cols), bf16),
        ((n_z, 2 * cap, feat), bf16),
        ((n_z, cap, feat), bf16),
        ((n_z, r_rows, feat), bf16),
        ((n_z + 1, r_rows, feat), bf16),
        ((r_rows, feat), f32),
        ((n_tp, 8, r_rows), f32),
        ((n_z, 8, r_rows), f32),
        ((n_z, 8, r_rows), f32),
        ((d_loc, h_cols), f32),
    ]
    sems = [
        (3, n_fs), (n_tp,), (n_tp,), (n_z,), (n_z,), (n_z,), (n_z,), (n_z,),
        (n_fs,), (n_fs,), (n_fs,), (n_fs,), (n_z,), (n_z,),
        (n_z,), (n_z,), (n_z,), (n_z,), (n_z,), (n_z,),
        (n_z,), (n_z,), (n_z,), (n_z,), (n_z,), (n_z,),
        (n_fs,), (per_quarter, n_tp), (n_z,), (n_z,), (n_z,), (n_z,), (n_z + 1,), (3, n_fs),
    ]
    return buffers, sems


def dims_of(tokens, gate_master, routes):
    n_fs, n_tp = lax.axis_size("fs"), lax.axis_size("tp")
    n_experts, d_loc, h_cols = gate_master.shape
    r_rows, top_count = routes.shape
    cap = 2 * r_rows * top_count // n_experts
    return (n_fs, n_tp, n_fs // PAIR, r_rows, tokens.shape[1], d_loc, h_cols, cap)


def fits(dims, n_experts, top_count):
    n_fs, n_tp, n_z, r_rows, feat, d_loc, h_cols, cap = dims
    if n_experts != n_fs or n_fs % PAIR or n_tp != 2 * PAIR or n_z != 2 * PAIR:
        return False
    if feat % d_loc or cap % 16 or h_cols % 128 or r_rows % 128 or d_loc % 128:
        return False
    total = 4 * r_rows * feat
    for shape, kind in scratch_for(dims)[0]:
        size = jnp.dtype(kind).itemsize
        for extent in shape:
            size = size * extent
        total = total + size
    return total < VMEM_BUDGET * 9 // 10


def body(tokens, gate_master, up_master, down_master, norm_gain, routes, route_weight):
    dims = dims_of(tokens, gate_master, routes)
    if not fits(dims, gate_master.shape[0], routes.shape[1]):
        return plain_body(tokens, gate_master, up_master, down_master, norm_gain, routes, route_weight)
    n_fs, n_tp, n_z, r_rows, feat, d_loc, h_cols, cap = dims
    buffers, sems = scratch_for(dims)
    vmem, anywhere = pl.BlockSpec(memory_space=pltpu.VMEM), pl.BlockSpec(memory_space=pl.ANY)
    matrix = jax.ShapeDtypeStruct((n_fs * d_loc, h_cols), jnp.bfloat16)
    gate_out, up_out, down_out, mixed = pl.pallas_call(
        functools.partial(moe_kernel, dims),
        out_shape=(matrix, matrix, matrix, jax.ShapeDtypeStruct((r_rows, feat), jnp.bfloat16)),
        in_specs=[vmem] * 4 + [anywhere] * 3,
        out_specs=(anywhere, anywhere, anywhere, vmem),
        scratch_shapes=[pltpu.VMEM(shape, kind) for shape, kind in buffers]
        + [pltpu.SemaphoreType.DMA(shape) for shape in sems],
        compiler_params=pltpu.CompilerParams(
            collective_id=0, has_side_effects=True, vmem_limit_bytes=VMEM_BUDGET
        ),
        name="experts",
    )(tokens, norm_gain[None, :], routes.T, route_weight.T, gate_master, up_master, down_master)
    return (gate_out[None], up_out[None], down_out[None], mixed)


def solution(mesh):
    placed = (
        P("fs", "tp"),
        P(None, "fs", "tp"),
        P(None, "fs", "tp"),
        P(None, "fs", "tp"),
        P("fs"),
        P("fs", None),
        P("fs", None),
    )
    return jax.shard_map(
        body,
        mesh=mesh,
        in_specs=placed,
        out_specs=(P("fs", None, "tp"), P("fs", None, "tp"), P("fs", None, "tp"), P("fs", "tp")),
        check_vma=False,
    )
```

```python
import functools

import jax
import jax.numpy as jnp
from jax import lax
from jax.experimental import pallas as pl
from jax.experimental.pallas import tpu as pltpu
from jax.sharding import PartitionSpec as P

norm_eps = 1e-06


def half_shift(step, size):
    half = size // 2
    return [(s, s // half * half + (s % half + step) % half) for s in range(size)]


def cross_swap(size):
    return [(s, (s + size // 2) % size) for s in range(size)]


def member_shift(step, crossed, size):
    half = size // 2
    return [
        (s, (s // half + crossed) % 2 * half + (s % half + step) % half) for s in range(size)
    ]


def plain_body(tokens, gate_master, up_master, down_master, norm_gain, routes, route_weight):
    n_experts = gate_master.shape[0]
    tok_rows, top_count = routes.shape
    capacity = 2 * tok_rows * top_count // n_experts
    n_tp = lax.axis_size("tp")
    half = n_tp // 2
    width = tokens.shape[1]
    hidden_cols = gate_master.shape[2]
    me_tp = lax.axis_index("tp")
    chunks = 2 if capacity % 32 == 0 else 1
    part = capacity // chunks

    folded = norm_gain[None, :, None]
    trio = jnp.concatenate(
        [
            (gate_master * folded).astype(jnp.bfloat16),
            (up_master * folded).astype(jnp.bfloat16),
            down_master.astype(jnp.bfloat16),
        ],
        axis=2,
    )
    trio = lax.all_to_all(trio, "fs", split_axis=0, concat_axis=1, tiled=True)
    pair = trio[:, :, : 2 * hidden_cols]
    gate_out = trio[:, :, :hidden_cols]
    up_out = trio[:, :, hidden_cols : 2 * hidden_cols]
    down_out = trio[:, :, 2 * hidden_cols :]

    token_float = tokens.astype(jnp.float32)
    sumsquares = lax.psum(jnp.sum(token_float * token_float, axis=1), "tp")
    inverse = lax.rsqrt(sumsquares / (width * n_tp) + norm_eps)[:, None]
    normed = (token_float * inverse).astype(jnp.bfloat16)
    mix = route_weight / jnp.sum(route_weight, axis=1, keepdims=True)
    experts = jnp.arange(n_experts, dtype=jnp.int32)
    named = jnp.any(routes[:, :, None] == experts, axis=1)
    earlier = jnp.arange(tok_rows)[:, None] > jnp.arange(tok_rows)[None, :]
    before = jnp.dot(
        earlier.astype(jnp.bfloat16), named.astype(jnp.bfloat16), preferred_element_type=jnp.float32
    ).astype(jnp.int32)
    slots = jnp.sum(jnp.where(routes[:, :, None] == experts, before[:, None, :], 0), axis=2)
    place = (slots // part * n_experts + routes) * part + slots % part
    spots = jnp.arange(n_experts * capacity, dtype=jnp.int32)
    where_to = place[:, :, None] == spots
    onehot = jnp.any(where_to, axis=1).astype(jnp.bfloat16)
    mixing = jnp.sum(jnp.where(where_to, mix[:, :, None], 0.0), axis=1)
    mixing = mixing.astype(jnp.bfloat16)
    outgoing = lax.dot_general(
        onehot, normed, (((0,), (0,)), ((), ())), preferred_element_type=jnp.float32
    ).astype(jnp.bfloat16)
    outgoing = outgoing.reshape(chunks, n_experts, part, width)

    my_half = me_tp // half
    inside = me_tp % half
    span = half * width
    own_cols = lax.dynamic_slice_in_dim(pair[0], my_half * span, span, 0)
    partner_cols = lax.ppermute(
        lax.dynamic_slice_in_dim(pair[0], (1 - my_half) * span, span, 0), "tp", cross_swap(n_tp)
    )

    arrived = []
    for c in range(chunks):
        if c == 0:
            ready, trio = lax.optimization_barrier((outgoing[c], trio))
        else:
            ready, arrived[-1], partner_cols = lax.optimization_barrier((outgoing[c], last, partner_cols))
        last = lax.all_to_all(ready, "fs", split_axis=0, concat_axis=0, tiled=True)
        arrived.append(last)

    def in_order(cols):
        blocks = cols.reshape(half, width, cols.shape[1])
        return [
            lax.dynamic_index_in_dim(blocks, (inside + half - j) % half, 0, keepdims=False)
            for j in range(half)
        ]

    own_blocks, partner_blocks = in_order(own_cols), in_order(partner_cols)
    quarters = down_out[0].reshape(n_tp, -1, hidden_cols)
    picked = []
    for j in range(half):
        for crossed in range(2):
            target = (my_half + crossed) % 2 * half + (inside + j) % half
            piece = lax.dynamic_index_in_dim(quarters, target, 0, keepdims=False)
            if j + crossed > 0:
                piece = lax.ppermute(piece, "tp", member_shift(j, crossed, n_tp))
            picked.append(piece)
    down_mat = jnp.concatenate(picked, axis=1)

    def serve(rows):
        rows = rows.reshape(-1, width)
        pieces = [rows] + [lax.ppermute(rows, "tp", half_shift(j, n_tp)) for j in range(1, half)]

        def partial(blocks):
            total = 0.0
            for piece, block in zip(pieces, blocks):
                total = total + jnp.dot(piece, block, preferred_element_type=jnp.float32)
            return total

        swapped = lax.ppermute(partial(partner_blocks).astype(jnp.bfloat16), "tp", cross_swap(n_tp))
        both = partial(own_blocks) + swapped.astype(jnp.float32)
        hidden = (jax.nn.silu(both[:, :hidden_cols]) * both[:, hidden_cols:]).astype(jnp.bfloat16)
        two = jnp.concatenate([hidden, lax.ppermute(hidden, "tp", cross_swap(n_tp))], axis=1)
        all_hidden = [two] + [lax.ppermute(two, "tp", half_shift(j, n_tp)) for j in range(1, half)]
        result = lax.dot_general(
            jnp.concatenate(all_hidden, axis=1),
            down_mat,
            (((1,), (1,)), ((), ())),
            preferred_element_type=jnp.float32,
        )
        return result.astype(jnp.bfloat16).reshape(-1, part, width)

    returned = []
    for c in range(chunks):
        rows = arrived[c]
        if c > 0:
            rows, served = lax.optimization_barrier((rows, served))
            returned.append(lax.all_to_all(served, "fs", split_axis=0, concat_axis=0, tiled=True))
        served = serve(rows)
    returned.append(lax.all_to_all(served, "fs", split_axis=0, concat_axis=0, tiled=True))

    mixed = 0.0
    for c, back in enumerate(returned):
        flat = back.reshape(n_experts * part, width)
        chosen = mixing[:, c * n_experts * part : (c + 1) * n_experts * part]
        mixed = mixed + jnp.dot(chosen, flat, preferred_element_type=jnp.float32)
    return (gate_out, up_out, down_out, mixed.astype(jnp.bfloat16))


PAIR = 2
VMEM_BUDGET = 62 * 1024 * 1024


def near_first(n_z):
    return [sorted(range(n_z), key=lambda b: (abs(b - z), b)) for z in range(n_z)]


def far_first(n_z):
    def rank(z, b):
        return (-abs(b - z), min(b, n_z - 1 - b), b)

    return [sorted(range(n_z), key=lambda b: rank(z, b)) for z in range(n_z)]


def looked_up(table, z, step):
    chosen = 0
    for i, row in enumerate(table):
        for s, value in enumerate(row):
            chosen = chosen + jnp.where((z == i) & (step == s), value, 0)
    return chosen


def moe_kernel(
    dims,
    tok, gain, routes, weight, gate_hbm, up_hbm, down_hbm,
    gate_out, up_out, down_out, mixed_out,
    stage, wgu_send, wd_send, wgu_recv, wd_recv, blk, rows, xsend, hid, dn, yb, ysend,
    rs_send, rs_recv, acc, ssq, aux_send, aux_recv, gain_mat,
    stage_sem, ssq_s, ssq_r, aux_s, aux_r, ag_sr, ag_sl, ag_r,
    wgu_s, wgu_r, wd_s, wd_r, x_s, x_r,
    rc_s, rc_r, ry_s, ry_r, rf_s, rf_r,
    hc_s, hc_r, hy_s, hy_r, hf_s, hf_r,
    dn_s, dn_r, y_s, y_r, rs_sr, rs_sl, rs_r, out_sem,
):
    n_fs, n_tp, n_z, r_rows, feat, d_loc, h_cols, cap = dims
    top_count = routes.shape[0]
    f32, bf16 = jnp.float32, jnp.bfloat16
    me = lax.axis_index("fs")
    t = lax.axis_index("tp")
    z, x = me // PAIR, me % PAIR
    xp = me - x + (1 - x)
    half = n_tp // 2
    tc = (t // half) * half + (half - 1 - t % half)
    ty = (t + half) % n_tp
    near, far = near_first(n_z), far_first(n_z)
    per_quarter = feat // d_loc

    def remote(src, dst, ssem, rsem, **where):
        return pltpu.make_async_remote_copy(
            src_ref=src, dst_ref=dst, send_sem=ssem, recv_sem=rsem,
            device_id=where, device_id_type=pl.DeviceIdType.MESH,
        )

    masters = (gate_hbm, up_hbm, down_hbm)

    def load(i, e):
        return pltpu.make_async_copy(masters[i].at[e], stage.at[i, e], stage_sem.at[i, e])

    def every(count, body):
        def step(i, carry):
            body(i)
            return carry
        lax.fori_loop(0, count, step, 0)

    barrier = pltpu.get_barrier_semaphore()
    for d in range(1, n_fs):
        pl.semaphore_signal(barrier, inc=1, device_id={"fs": (me + d) % n_fs},
                            device_id_type=pl.DeviceIdType.MESH)
    for d in range(1, n_tp):
        pl.semaphore_signal(barrier, inc=1, device_id={"tp": (t + d) % n_tp},
                            device_id_type=pl.DeviceIdType.MESH)

    def start_load(d):
        for i in range(3):
            load(i, (me + d) % n_fs).start()
    every(n_fs, start_load)

    blk[z] = tok[...]

    value = tok[...].astype(f32)
    column = jnp.sum(value * value, axis=1, keepdims=True)
    spread = jnp.transpose(jnp.broadcast_to(column, (r_rows, 128)))
    ssq[t] = spread[:8]

    with jax.named_scope("bar"):
        pl.semaphore_wait(barrier, n_fs - 1 + n_tp - 1)

    def ssq_copy(d):
        peer = (t + d) % n_tp
        return remote(ssq.at[t], ssq.at[t], ssq_s.at[d], ssq_r.at[t], tp=peer)

    def ssq_from(d):
        peer = (t + n_tp - d) % n_tp
        return remote(ssq.at[peer], ssq.at[peer], ssq_s.at[d], ssq_r.at[peer], tp=peer)
    for d in range(1, n_tp):
        ssq_copy(d).start()

    def ag_right(b):
        return remote(blk.at[b], blk.at[b], ag_sr.at[b], ag_r.at[b], fs=me + PAIR)

    def ag_left(b):
        return remote(blk.at[b], blk.at[b], ag_sl.at[b], ag_r.at[b], fs=me - PAIR)

    def goes_right(b):
        return (b <= z) & (z < n_z - 1)

    def goes_left(b):
        return (b >= z) & (z > 0)

    def ag_start(b):
        @pl.when(goes_right(b))
        def _():
            ag_right(b).start()

        @pl.when(goes_left(b))
        def _():
            ag_left(b).start()
    ag_start(z)

    expert = lax.broadcasted_iota(jnp.int32, (n_fs, r_rows), 0)
    picks = [jnp.broadcast_to(routes[k : k + 1, :], (n_fs, r_rows)) == expert for k in range(top_count)]
    weights = weight[...]
    mix = weights / jnp.sum(weights, axis=0, keepdims=True)
    named = jnp.zeros((n_fs, r_rows), f32)
    mixed_t = jnp.zeros((n_fs, r_rows), f32)
    for k in range(top_count):
        named = named + jnp.where(picks[k], 1.0, 0.0)
        mixed_t = mixed_t + jnp.where(picks[k], jnp.broadcast_to(mix[k : k + 1, :], (n_fs, r_rows)), 0.0)
    first = lax.broadcasted_iota(jnp.int32, (r_rows, r_rows), 0)
    second = lax.broadcasted_iota(jnp.int32, (r_rows, r_rows), 1)
    earlier = jnp.where(first < second, 1.0, 0.0).astype(bf16)
    before = jnp.dot(named.astype(bf16), earlier, preferred_element_type=f32)
    slot_t = jnp.where(named > 0.0, before, -1.0)
    with jax.named_scope("ssqwait"):
        for d in range(1, n_tp):
            ssq_from(d).wait_recv()
    total = ssq[0]
    for k in range(1, n_tp):
        total = total + ssq[k]
    inverse = lax.rsqrt(total / (feat * n_tp) + norm_eps)
    for plane in range(n_z):
        lo = plane * PAIR
        aux_send[plane, 0:PAIR, :] = slot_t[lo : lo + PAIR]
        aux_send[plane, PAIR : 2 * PAIR, :] = mixed_t[lo : lo + PAIR]
        aux_send[plane, 2 * PAIR :, :] = inverse[2 * PAIR :]
    aux_recv[z] = aux_send[z]

    def aux_copy(d):
        plane = (z + d) % n_z
        return remote(aux_send.at[plane], aux_recv.at[z], aux_s.at[d], aux_r.at[z], fs=plane * PAIR + x)

    def aux_from(plane):
        return remote(aux_send.at[plane], aux_recv.at[plane], aux_s.at[0], aux_r.at[plane], fs=me)
    for d in range(1, n_z):
        aux_copy(d).start()

    gain_mat[...] = jnp.transpose(jnp.broadcast_to(gain[...], (h_cols, d_loc)))

    def wgu_copy(d):
        e = (me + d) % n_fs
        return remote(wgu_send.at[e], wgu_recv.at[me], wgu_s.at[d], wgu_r.at[me], fs=e)

    def wgu_from(j):
        return remote(wgu_send.at[j], wgu_recv.at[j], wgu_s.at[0], wgu_r.at[j], fs=me)

    def wd_copy(d):
        e = (me + d) % n_fs
        return remote(wd_send.at[e], wd_recv.at[me], wd_s.at[d], wd_r.at[me], fs=e)

    def wd_from(j):
        return remote(wd_send.at[j], wd_recv.at[j], wd_s.at[0], wd_r.at[j], fs=me)

    def cast_gu(d, target, index):
        e = (me + d) % n_fs
        load(0, e).wait()
        load(1, e).wait()
        target[index, :, 0:h_cols] = (stage[0, e] * gain_mat[...]).astype(bf16)
        target[index, :, h_cols : 2 * h_cols] = (stage[1, e] * gain_mat[...]).astype(bf16)

    def cast_d(d, target, index):
        e = (me + d) % n_fs
        load(2, e).wait()
        target[index] = stage[2, e].astype(bf16)

    def send_gu(d):
        cast_gu(d, wgu_send, (me + d) % n_fs)
        wgu_copy(d).start()

    def send_d(d):
        cast_d(d, wd_send, (me + d) % n_fs)
        wd_copy(d).start()

    def span(first_d, last_d, body):
        every(last_d - first_d, lambda i: body(i + first_d))

    def picker(b, which):
        slots = aux_recv[b, pl.ds(which, 1), :]
        at = lax.broadcasted_iota(jnp.int32, (cap, r_rows), 0).astype(f32)
        return at == jnp.broadcast_to(slots, (cap, r_rows))

    def x_copy(b):
        return remote(xsend.at[b], rows.at[t, b, pl.ds(cap, cap)], x_s.at[b], x_r.at[b], fs=xp)

    def stage_a(s):
        b = looked_up(near, z, s)

        @pl.when(b != z)
        def _():
            ag_right(b).wait_recv()
            ag_start(b)
            aux_from(b).wait_recv()
        scale = jnp.broadcast_to(aux_recv[b, 2 * PAIR : 2 * PAIR + 1, :], (cap, r_rows))

        def compact(which):
            hit = picker(b, which)
            factor = jnp.sum(jnp.where(hit, scale, 0.0), axis=1, keepdims=True)
            taken = jnp.dot(jnp.where(hit, 1.0, 0.0).astype(bf16), blk[b], preferred_element_type=f32)
            return (taken * factor).astype(bf16)
        xsend[b] = compact(1 - x)
        x_copy(b).start()
        rows[t, b, 0:cap, :] = compact(x)

    def rc_copy(b):
        return remote(rows.at[t, b], rows.at[t, b], rc_s.at[b], rc_r.at[b], tp=tc)

    def ry_copy(b):
        return remote(rows.at[t, b], rows.at[t, b], ry_s.at[b], ry_r.at[b], tp=ty)

    def rf_copy(b):
        return remote(rows.at[ty, b], rows.at[ty, b], rf_s.at[b], rf_r.at[b], tp=tc)

    def stage_b(s):
        b = looked_up(near, z, s)
        x_copy(b).wait_recv()
        ry_copy(b).start()
        rc_copy(b).start()

    def stage_c(s):
        b = looked_up(near, z, s)
        ry_copy(b).wait_recv()
        rf_copy(b).start()

    def plane_sends(plane, body):
        for k in range(PAIR):
            body((plane * PAIR + k + n_fs - me) % n_fs)

    def side_sends(to_right, body):
        for d in range(1, n_z):
            if to_right:
                @pl.when(z + d < n_z)
                def _():
                    plane_sends(z + d, body)
            else:
                @pl.when(z >= d)
                def _():
                    plane_sends(z - d, body)

    def shorter_side(body):
        right = z < n_z // 2

        @pl.when(right)
        def _():
            side_sends(False, body)

        @pl.when(~right)
        def _():
            side_sends(True, body)

    inner = (z > 0) & (z < n_z - 1)

    def partner_sends(body):
        body((xp + n_fs - me) % n_fs)

    def named(kind, s):
        with jax.named_scope(kind + str(s)):
            {"a": stage_a, "b": stage_b, "c": stage_c}[kind](s)

    def run(*steps):
        for step in steps:
            if isinstance(step, str):
                named(step[0], int(step[1]))
            else:
                with jax.named_scope("w"):
                    step()

    def toward(distance, body):
        @pl.when(z < n_z // 2)
        def _():
            plane_sends(z + distance, body)

        @pl.when(z >= n_z // 2)
        def _():
            plane_sends(z - distance, body)

    def forwarded():
        @pl.when(z < n_z // 2)
        def _():
            ag_left(z + 2).wait_send()

        @pl.when(z >= n_z // 2)
        def _():
            ag_right(z - 2).wait_send()

    def partner_all():
        partner_sends(send_gu)
        partner_sends(send_d)

    def inner_second():
        forwarded()
        toward(2, send_gu)
        shorter_side(send_gu)

    def inner_third():
        toward(1, send_d)
        toward(2, send_d)
        shorter_side(send_d)

    def outer_first():
        toward(1, send_gu)
        toward(1, send_d)

    def outer_third():
        toward(2, send_d)
        toward(3, send_d)

    @pl.when(inner)
    def _():
        run("a0", partner_all, "b0", "a1", "a2", "b1", "c0", "a3", lambda: toward(1, send_gu),
            "b2", "c1", inner_second, "b3", "c2", inner_third)

    @pl.when(~inner)
    def _():
        run("a0", partner_all, "b0", "a1", outer_first, "b1", "c0", "a2", lambda: toward(2, send_gu),
            "b2", "c1", "a3", lambda: toward(3, send_gu), "b3", "c2", outer_third)
    cast_gu(0, wgu_recv, me)
    cast_d(0, wd_recv, me)
    with jax.named_scope("c3"):
        stage_c(3)

    def wait_gu(d):
        wgu_from((me + n_fs - d) % n_fs).wait_recv()
    with jax.named_scope("span_1_n_fs_wait_gu_"):
        span(1, n_fs, wait_gu)

    def hc_copy(b):
        return remote(hid.at[t, b], hid.at[t, b], hc_s.at[b], hc_r.at[b], tp=tc)

    def hy_copy(b):
        return remote(hid.at[t, b], hid.at[t, b], hy_s.at[b], hy_r.at[b], tp=ty)

    def hf_copy(b):
        return remote(hid.at[ty, b], hid.at[ty, b], hf_s.at[b], hf_r.at[b], tp=tc)

    def stage_d(s):
        b = looked_up(far, z, s)
        rc_copy(b).wait_recv()
        rf_copy(b).wait_recv()
        both = jnp.zeros((2 * cap, 2 * h_cols), f32)
        for j in range(n_fs):
            lo = (j % per_quarter) * d_loc
            both = both + jnp.dot(rows[j // per_quarter, b, :, lo : lo + d_loc], wgu_recv[j],
                                  preferred_element_type=f32)
        gates = both[:, 0:h_cols]
        hid[t, b] = (gates / (1.0 + jnp.exp(-gates)) * both[:, h_cols:]).astype(bf16)
        hy_copy(b).start()
        hc_copy(b).start()
    with jax.named_scope("every_n_z_stage_d_"):
        every(n_z, stage_d)

    def out_copies(j):
        at = pl.ds(pl.multiple_of(j * d_loc, d_loc), d_loc)
        return [
            pltpu.make_async_copy(wgu_recv.at[j, :, pl.ds(0, h_cols)], gate_out.at[at], out_sem.at[0, j]),
            pltpu.make_async_copy(wgu_recv.at[j, :, pl.ds(h_cols, h_cols)], up_out.at[at], out_sem.at[1, j]),
            pltpu.make_async_copy(wd_recv.at[j], down_out.at[at], out_sem.at[2, j]),
        ]

    def dn_copy(j):
        q = j % per_quarter
        return remote(wd_recv.at[j], dn.at[q, t], dn_s.at[j], dn_r.at[q, t], tp=j // per_quarter)

    def dn_from(q, k):
        return remote(wd_recv.at[0], dn.at[q, k], dn_s.at[0], dn_r.at[q, k], tp=t)

    def pass_down(j):
        @pl.when(j != me)
        def _():
            wd_from(j).wait_recv()

        @pl.when(j // per_quarter == t)
        def _():
            dn[j % per_quarter, t] = wd_recv[j]

        @pl.when(j // per_quarter != t)
        def _():
            dn_copy(j).start()
        for copy in out_copies(j):
            copy.start()

    def pass_planes(first_s, last_s):
        def one(s):
            plane = looked_up(near, z, s)
            for k in range(PAIR):
                pass_down(plane * PAIR + k)
        span(first_s, last_s, one)
    with jax.named_scope("pass_near"):
        pass_planes(0, n_z // 2)

    def stage_e(s):
        b = looked_up(far, z, s)
        hy_copy(b).wait_recv()
        hf_copy(b).start()
    with jax.named_scope("every_n_z_stage_e_"):
        every(n_z, stage_e)
    with jax.named_scope("pass_far"):
        pass_planes(n_z // 2, n_z)

    def wait_dn(d):
        k = (t + d) % n_tp
        for q in range(per_quarter):
            dn_from(q, k).wait_recv()
    with jax.named_scope("span_1_n_tp_wait_dn_"):
        span(1, n_tp, wait_dn)

    def y_copy(b, q):
        return remote(ysend.at[b, q], yb.at[b, q, pl.ds(cap, cap)], y_s.at[b, q], y_r.at[b, q], fs=xp)

    def stage_f(s):
        b = looked_up(far, z, s)
        hc_copy(b).wait_recv()
        hf_copy(b).wait_recv()
        units = jnp.concatenate([hid[k, b] for k in range(n_tp)], axis=1)
        for q in range(per_quarter):
            mat = jnp.concatenate([dn[q, k] for k in range(n_tp)], axis=1)
            result = lax.dot_general(units, mat, (((1,), (1,)), ((), ())), preferred_element_type=f32)
            result = result.astype(bf16)
            ysend[b, q] = result[cap:]
            y_copy(b, q).start()
            yb[b, q, 0:cap, :] = result[:cap]
    with jax.named_scope("every_n_z_stage_f_"):
        every(n_z, stage_f)

    def rs_right(b, q):
        return remote(rs_send.at[b, q], rs_recv.at[b, q], rs_sr.at[b, q], rs_r.at[b, q], fs=me + PAIR)

    def rs_left(b, q):
        at = jnp.where(b == z - 1, n_z, b)
        return remote(rs_send.at[b, q], rs_recv.at[at, q], rs_sl.at[b, q], rs_r.at[at, q], fs=me - PAIR)

    def rs_from(at, q):
        return remote(rs_send.at[0, q], rs_recv.at[at, q], rs_sr.at[0, q], rs_r.at[at, q], fs=me)

    def stage_g(s):
        b = looked_up(far, z, s)

        def share(which):
            weights = jnp.broadcast_to(aux_recv[b, pl.ds(PAIR + which, 1), :], (cap, r_rows))
            return jnp.where(picker(b, which), weights, 0.0).astype(bf16)
        spreading = jnp.concatenate([share(x), share(1 - x)], axis=0)
        for q in range(per_quarter):
            y_copy(b, q).wait_recv()
            acc[...] = lax.dot_general(spreading, yb[b, q], (((0,), (0,)), ((), ())), preferred_element_type=f32)

            @pl.when(((b >= z) & (z > 0)) | ((b < z) & (z < n_z - 1)))
            def _():
                rs_from(b, q).wait_recv()
                acc[...] += rs_recv[b, q].astype(f32)

            @pl.when((b == z) & (z < n_z - 1))
            def _():
                rs_from(n_z, q).wait_recv()
                acc[...] += rs_recv[n_z, q].astype(f32)

            @pl.when(b != z)
            def _():
                rs_send[b, q] = acc[...].astype(bf16)

            @pl.when(b > z)
            def _():
                rs_right(b, q).start()

            @pl.when(b < z)
            def _():
                rs_left(b, q).start()

            @pl.when(b == z)
            def _():
                mixed_out[:, q * d_loc : (q + 1) * d_loc] = acc[...].astype(bf16)
    with jax.named_scope("every_n_z_stage_g_"):
        every(n_z, stage_g)

    for d in range(1, n_tp):
        ssq_copy(d).wait_send()
    for d in range(1, n_z):
        aux_copy(d).wait_send()

    def sent_w(d):
        wgu_copy(d).wait_send()
        wd_copy(d).wait_send()
    span(1, n_fs, sent_w)

    def sent_b(b):
        @pl.when(goes_right(b) & ~(inner & (b == z - 2)))
        def _():
            ag_right(b).wait_send()

        @pl.when(goes_left(b) & ~(inner & (b == z + 2)))
        def _():
            ag_left(b).wait_send()
        for copy in (x_copy, rc_copy, ry_copy, rf_copy, hc_copy, hy_copy, hf_copy):
            copy(b).wait_send()
        for q in range(per_quarter):
            y_copy(b, q).wait_send()

            @pl.when(b > z)
            def _():
                rs_right(b, q).wait_send()

            @pl.when(b < z)
            def _():
                rs_left(b, q).wait_send()
    every(n_z, sent_b)

    def sent_j(j):
        @pl.when(j // per_quarter != t)
        def _():
            dn_copy(j).wait_send()
        for copy in out_copies(j):
            copy.wait()
    every(n_fs, sent_j)


def scratch_for(dims):
    n_fs, n_tp, n_z, r_rows, feat, d_loc, h_cols, cap = dims
    f32, bf16 = jnp.float32, jnp.bfloat16
    per_quarter = feat // d_loc
    buffers = [
        ((3, n_fs, d_loc, h_cols), f32),
        ((n_fs, d_loc, 2 * h_cols), bf16),
        ((n_fs, d_loc, h_cols), bf16),
        ((n_fs, d_loc, 2 * h_cols), bf16),
        ((n_fs, d_loc, h_cols), bf16),
        ((n_z, r_rows, feat), bf16),
        ((n_tp, n_z, 2 * cap, feat), bf16),
        ((n_z, cap, feat), bf16),
        ((n_tp, n_z, 2 * cap, h_cols), bf16),
        ((per_quarter, n_tp, d_loc, h_cols), bf16),
        ((n_z, per_quarter, 2 * cap, d_loc), bf16),
        ((n_z, per_quarter, cap, d_loc), bf16),
        ((n_z, per_quarter, r_rows, d_loc), bf16),
        ((n_z + 1, per_quarter, r_rows, d_loc), bf16),
        ((r_rows, d_loc), f32),
        ((n_tp, 8, r_rows), f32),
        ((n_z, 8, r_rows), f32),
        ((n_z, 8, r_rows), f32),
        ((d_loc, h_cols), f32),
    ]
    sems = [
        (3, n_fs), (n_tp,), (n_tp,), (n_z,), (n_z,), (n_z,), (n_z,), (n_z,),
        (n_fs,), (n_fs,), (n_fs,), (n_fs,), (n_z,), (n_z,),
        (n_z,), (n_z,), (n_z,), (n_z,), (n_z,), (n_z,),
        (n_z,), (n_z,), (n_z,), (n_z,), (n_z,), (n_z,),
        (n_fs,), (per_quarter, n_tp), (n_z, per_quarter), (n_z, per_quarter),
        (n_z, per_quarter), (n_z, per_quarter), (n_z + 1, per_quarter), (3, n_fs),
    ]
    return buffers, sems


def dims_of(tokens, gate_master, routes):
    n_fs, n_tp = lax.axis_size("fs"), lax.axis_size("tp")
    n_experts, d_loc, h_cols = gate_master.shape
    r_rows, top_count = routes.shape
    cap = 2 * r_rows * top_count // n_experts
    return (n_fs, n_tp, n_fs // PAIR, r_rows, tokens.shape[1], d_loc, h_cols, cap)


def fits(dims, n_experts, top_count):
    n_fs, n_tp, n_z, r_rows, feat, d_loc, h_cols, cap = dims
    if n_experts != n_fs or n_fs % PAIR or n_tp != 2 * PAIR or n_z != 2 * PAIR:
        return False
    if feat % d_loc or cap % 16 or h_cols % 128 or r_rows % 128 or d_loc % 128:
        return False
    total = 4 * r_rows * feat
    for shape, kind in scratch_for(dims)[0]:
        size = jnp.dtype(kind).itemsize
        for extent in shape:
            size = size * extent
        total = total + size
    return total < VMEM_BUDGET * 9 // 10


def body(tokens, gate_master, up_master, down_master, norm_gain, routes, route_weight):
    dims = dims_of(tokens, gate_master, routes)
    if not fits(dims, gate_master.shape[0], routes.shape[1]):
        return plain_body(tokens, gate_master, up_master, down_master, norm_gain, routes, route_weight)
    n_fs, n_tp, n_z, r_rows, feat, d_loc, h_cols, cap = dims
    buffers, sems = scratch_for(dims)
    vmem, anywhere = pl.BlockSpec(memory_space=pltpu.VMEM), pl.BlockSpec(memory_space=pl.ANY)
    matrix = jax.ShapeDtypeStruct((n_fs * d_loc, h_cols), jnp.bfloat16)
    gate_out, up_out, down_out, mixed = pl.pallas_call(
        functools.partial(moe_kernel, dims),
        out_shape=(matrix, matrix, matrix, jax.ShapeDtypeStruct((r_rows, feat), jnp.bfloat16)),
        in_specs=[vmem] * 4 + [anywhere] * 3,
        out_specs=(anywhere, anywhere, anywhere, vmem),
        scratch_shapes=[pltpu.VMEM(shape, kind) for shape, kind in buffers]
        + [pltpu.SemaphoreType.DMA(shape) for shape in sems],
        compiler_params=pltpu.CompilerParams(
            collective_id=0, has_side_effects=True, vmem_limit_bytes=VMEM_BUDGET
        ),
        name="experts",
    )(tokens, norm_gain[None, :], routes.T, route_weight.T, gate_master, up_master, down_master)
    return (gate_out[None], up_out[None], down_out[None], mixed)


def solution(mesh):
    placed = (
        P("fs", "tp"),
        P(None, "fs", "tp"),
        P(None, "fs", "tp"),
        P(None, "fs", "tp"),
        P("fs"),
        P("fs", None),
        P("fs", None),
    )
    return jax.shard_map(
        body,
        mesh=mesh,
        in_specs=placed,
        out_specs=(P("fs", None, "tp"), P("fs", None, "tp"), P("fs", None, "tp"), P("fs", "tp")),
        check_vma=False,
    )
```

```python
import functools

import jax
import jax.numpy as jnp
from jax import lax
from jax.experimental import pallas as pl
from jax.experimental.pallas import tpu as pltpu
from jax.sharding import PartitionSpec as P

norm_eps = 1e-06


def half_shift(step, size):
    half = size // 2
    return [(s, s // half * half + (s % half + step) % half) for s in range(size)]


def cross_swap(size):
    return [(s, (s + size // 2) % size) for s in range(size)]


def member_shift(step, crossed, size):
    half = size // 2
    return [
        (s, (s // half + crossed) % 2 * half + (s % half + step) % half) for s in range(size)
    ]


def plain_body(tokens, gate_master, up_master, down_master, norm_gain, routes, route_weight):
    n_experts = gate_master.shape[0]
    tok_rows, top_count = routes.shape
    capacity = 2 * tok_rows * top_count // n_experts
    n_tp = lax.axis_size("tp")
    half = n_tp // 2
    width = tokens.shape[1]
    hidden_cols = gate_master.shape[2]
    me_tp = lax.axis_index("tp")
    chunks = 2 if capacity % 32 == 0 else 1
    part = capacity // chunks

    folded = norm_gain[None, :, None]
    trio = jnp.concatenate(
        [
            (gate_master * folded).astype(jnp.bfloat16),
            (up_master * folded).astype(jnp.bfloat16),
            down_master.astype(jnp.bfloat16),
        ],
        axis=2,
    )
    trio = lax.all_to_all(trio, "fs", split_axis=0, concat_axis=1, tiled=True)
    pair = trio[:, :, : 2 * hidden_cols]
    gate_out = trio[:, :, :hidden_cols]
    up_out = trio[:, :, hidden_cols : 2 * hidden_cols]
    down_out = trio[:, :, 2 * hidden_cols :]

    token_float = tokens.astype(jnp.float32)
    sumsquares = lax.psum(jnp.sum(token_float * token_float, axis=1), "tp")
    inverse = lax.rsqrt(sumsquares / (width * n_tp) + norm_eps)[:, None]
    normed = (token_float * inverse).astype(jnp.bfloat16)
    mix = route_weight / jnp.sum(route_weight, axis=1, keepdims=True)
    experts = jnp.arange(n_experts, dtype=jnp.int32)
    named = jnp.any(routes[:, :, None] == experts, axis=1)
    earlier = jnp.arange(tok_rows)[:, None] > jnp.arange(tok_rows)[None, :]
    before = jnp.dot(
        earlier.astype(jnp.bfloat16), named.astype(jnp.bfloat16), preferred_element_type=jnp.float32
    ).astype(jnp.int32)
    slots = jnp.sum(jnp.where(routes[:, :, None] == experts, before[:, None, :], 0), axis=2)
    place = (slots // part * n_experts + routes) * part + slots % part
    spots = jnp.arange(n_experts * capacity, dtype=jnp.int32)
    where_to = place[:, :, None] == spots
    onehot = jnp.any(where_to, axis=1).astype(jnp.bfloat16)
    mixing = jnp.sum(jnp.where(where_to, mix[:, :, None], 0.0), axis=1)
    mixing = mixing.astype(jnp.bfloat16)
    outgoing = lax.dot_general(
        onehot, normed, (((0,), (0,)), ((), ())), preferred_element_type=jnp.float32
    ).astype(jnp.bfloat16)
    outgoing = outgoing.reshape(chunks, n_experts, part, width)

    my_half = me_tp // half
    inside = me_tp % half
    span = half * width
    own_cols = lax.dynamic_slice_in_dim(pair[0], my_half * span, span, 0)
    partner_cols = lax.ppermute(
        lax.dynamic_slice_in_dim(pair[0], (1 - my_half) * span, span, 0), "tp", cross_swap(n_tp)
    )

    arrived = []
    for c in range(chunks):
        if c == 0:
            ready, trio = lax.optimization_barrier((outgoing[c], trio))
        else:
            ready, arrived[-1], partner_cols = lax.optimization_barrier((outgoing[c], last, partner_cols))
        last = lax.all_to_all(ready, "fs", split_axis=0, concat_axis=0, tiled=True)
        arrived.append(last)

    def in_order(cols):
        blocks = cols.reshape(half, width, cols.shape[1])
        return [
            lax.dynamic_index_in_dim(blocks, (inside + half - j) % half, 0, keepdims=False)
            for j in range(half)
        ]

    own_blocks, partner_blocks = in_order(own_cols), in_order(partner_cols)
    quarters = down_out[0].reshape(n_tp, -1, hidden_cols)
    picked = []
    for j in range(half):
        for crossed in range(2):
            target = (my_half + crossed) % 2 * half + (inside + j) % half
            piece = lax.dynamic_index_in_dim(quarters, target, 0, keepdims=False)
            if j + crossed > 0:
                piece = lax.ppermute(piece, "tp", member_shift(j, crossed, n_tp))
            picked.append(piece)
    down_mat = jnp.concatenate(picked, axis=1)

    def serve(rows):
        rows = rows.reshape(-1, width)
        pieces = [rows] + [lax.ppermute(rows, "tp", half_shift(j, n_tp)) for j in range(1, half)]

        def partial(blocks):
            total = 0.0
            for piece, block in zip(pieces, blocks):
                total = total + jnp.dot(piece, block, preferred_element_type=jnp.float32)
            return total

        swapped = lax.ppermute(partial(partner_blocks).astype(jnp.bfloat16), "tp", cross_swap(n_tp))
        both = partial(own_blocks) + swapped.astype(jnp.float32)
        hidden = (jax.nn.silu(both[:, :hidden_cols]) * both[:, hidden_cols:]).astype(jnp.bfloat16)
        two = jnp.concatenate([hidden, lax.ppermute(hidden, "tp", cross_swap(n_tp))], axis=1)
        all_hidden = [two] + [lax.ppermute(two, "tp", half_shift(j, n_tp)) for j in range(1, half)]
        result = lax.dot_general(
            jnp.concatenate(all_hidden, axis=1),
            down_mat,
            (((1,), (1,)), ((), ())),
            preferred_element_type=jnp.float32,
        )
        return result.astype(jnp.bfloat16).reshape(-1, part, width)

    returned = []
    for c in range(chunks):
        rows = arrived[c]
        if c > 0:
            rows, served = lax.optimization_barrier((rows, served))
            returned.append(lax.all_to_all(served, "fs", split_axis=0, concat_axis=0, tiled=True))
        served = serve(rows)
    returned.append(lax.all_to_all(served, "fs", split_axis=0, concat_axis=0, tiled=True))

    mixed = 0.0
    for c, back in enumerate(returned):
        flat = back.reshape(n_experts * part, width)
        chosen = mixing[:, c * n_experts * part : (c + 1) * n_experts * part]
        mixed = mixed + jnp.dot(chosen, flat, preferred_element_type=jnp.float32)
    return (gate_out, up_out, down_out, mixed.astype(jnp.bfloat16))


PAIR = 2
VMEM_BUDGET = 62 * 1024 * 1024


def near_first(n_z):
    return [sorted(range(n_z), key=lambda b: (abs(b - z), b)) for z in range(n_z)]


def far_first(n_z):
    def rank(z, b):
        return (-abs(b - z), -min(b, n_z - 1 - b), b)

    return [sorted(range(n_z), key=lambda b: rank(z, b)) for z in range(n_z)]


def looked_up(table, z, step):
    chosen = 0
    for i, row in enumerate(table):
        for s, value in enumerate(row):
            chosen = chosen + jnp.where((z == i) & (step == s), value, 0)
    return chosen


def moe_kernel(
    dims,
    tok, gain, routes, weight, gate_hbm, up_hbm, down_hbm,
    gate_out, up_out, down_out, mixed_out,
    stage, wgu_send, wd_send, wgu_recv, wd_recv, blk, rows, xsend, hid, dn, yb, ysend,
    rs_send, rs_recv, acc, both, wd2, dn2, hid2, yb2, ysend2, ssq, aux_send, aux_recv, gain_mat,
    stage_sem, ssq_s, ssq_r, aux_s, aux_r, ag_sr, ag_sl, ag_r,
    wgu_s, wgu_r, wd_s, wd_r, x_s, x_r,
    rc_s, rc_r, ry_s, ry_r, rf_s, rf_r,
    hc_s, hc_r, hy_s, hy_r, hf_s, hf_r,
    dn_s, dn_r, y_s, y_r, rs_sr, rs_sl, rs_r, out_sem,
    w2_s, w2_r, wf_s, d2_s, d2_r, h2_sem, y2_s, y2_r,
):
    n_fs, n_tp, n_z, r_rows, feat, d_loc, h_cols, cap = dims
    top_count = routes.shape[0]
    f32, bf16 = jnp.float32, jnp.bfloat16
    me = lax.axis_index("fs")
    t = lax.axis_index("tp")
    z, x = me // PAIR, me % PAIR
    xp = me - x + (1 - x)
    half = n_tp // 2
    tc = (t // half) * half + (half - 1 - t % half)
    ty = (t + half) % n_tp
    near, far = near_first(n_z), far_first(n_z)
    per_quarter = feat // d_loc

    def remote(src, dst, ssem, rsem, **where):
        return pltpu.make_async_remote_copy(
            src_ref=src, dst_ref=dst, send_sem=ssem, recv_sem=rsem,
            device_id=where, device_id_type=pl.DeviceIdType.MESH,
        )

    masters = (gate_hbm, up_hbm, down_hbm)

    def load(i, e):
        return pltpu.make_async_copy(masters[i].at[e], stage.at[i, e], stage_sem.at[i, e])

    def every(count, body):
        def step(i, carry):
            body(i)
            return carry
        lax.fori_loop(0, count, step, 0)

    barrier = pltpu.get_barrier_semaphore()
    for d in range(1, n_fs):
        pl.semaphore_signal(barrier, inc=1, device_id={"fs": (me + d) % n_fs},
                            device_id_type=pl.DeviceIdType.MESH)
    for d in range(1, n_tp):
        pl.semaphore_signal(barrier, inc=1, device_id={"tp": (t + d) % n_tp},
                            device_id_type=pl.DeviceIdType.MESH)

    def start_load(d):
        for i in range(3):
            load(i, (me + d) % n_fs).start()
    every(n_fs, start_load)

    blk[z] = tok[...]

    value = tok[...].astype(f32)
    column = jnp.sum(value * value, axis=1, keepdims=True)
    spread = jnp.transpose(jnp.broadcast_to(column, (r_rows, 128)))
    ssq[t] = spread[:8]

    with jax.named_scope("bar"):
        pl.semaphore_wait(barrier, n_fs - 1 + n_tp - 1)

    def ssq_copy(d):
        peer = (t + d) % n_tp
        return remote(ssq.at[t], ssq.at[t], ssq_s.at[d], ssq_r.at[t], tp=peer)

    def ssq_from(d):
        peer = (t + n_tp - d) % n_tp
        return remote(ssq.at[peer], ssq.at[peer], ssq_s.at[d], ssq_r.at[peer], tp=peer)
    for d in range(1, n_tp):
        ssq_copy(d).start()

    def ag_right(b):
        return remote(blk.at[b], blk.at[b], ag_sr.at[b], ag_r.at[b], fs=me + PAIR)

    def ag_left(b):
        return remote(blk.at[b], blk.at[b], ag_sl.at[b], ag_r.at[b], fs=me - PAIR)

    def goes_right(b):
        return (b <= z) & (z < n_z - 1)

    def goes_left(b):
        return (b >= z) & (z > 0)

    def ag_start(b):
        @pl.when(goes_right(b))
        def _():
            ag_right(b).start()

        @pl.when(goes_left(b))
        def _():
            ag_left(b).start()
    ag_start(z)

    side = jnp.where(z < n_z // 2, 1, -1)
    inner = (z > 0) & (z < n_z - 1)

    def at(distance):
        return z + side * distance

    def help_copy(k):
        src = wd_send.at[xp] if k == 0 else wd_recv.at[me]
        column = 1 - x if k == 0 else x
        return remote(src, wd2.at[me], w2_s.at[k], w2_r.at[me], fs=at(1) * PAIR + column)

    expert = lax.broadcasted_iota(jnp.int32, (n_fs, r_rows), 0)
    picks = [jnp.broadcast_to(routes[k : k + 1, :], (n_fs, r_rows)) == expert for k in range(top_count)]
    weights = weight[...]
    mix = weights / jnp.sum(weights, axis=0, keepdims=True)
    named = jnp.zeros((n_fs, r_rows), f32)
    mixed_t = jnp.zeros((n_fs, r_rows), f32)
    for k in range(top_count):
        named = named + jnp.where(picks[k], 1.0, 0.0)
        mixed_t = mixed_t + jnp.where(picks[k], jnp.broadcast_to(mix[k : k + 1, :], (n_fs, r_rows)), 0.0)
    first = lax.broadcasted_iota(jnp.int32, (r_rows, r_rows), 0)
    second = lax.broadcasted_iota(jnp.int32, (r_rows, r_rows), 1)
    earlier = jnp.where(first < second, 1.0, 0.0).astype(bf16)
    before = jnp.dot(named.astype(bf16), earlier, preferred_element_type=f32)
    slot_t = jnp.where(named > 0.0, before, -1.0)
    with jax.named_scope("ssqwait"):
        for d in range(1, n_tp):
            ssq_from(d).wait_recv()
    total = ssq[0]
    for k in range(1, n_tp):
        total = total + ssq[k]
    inverse = lax.rsqrt(total / (feat * n_tp) + norm_eps)
    for plane in range(n_z):
        lo = plane * PAIR
        aux_send[plane, 0:PAIR, :] = slot_t[lo : lo + PAIR]
        aux_send[plane, PAIR : 2 * PAIR, :] = mixed_t[lo : lo + PAIR]
        aux_send[plane, 2 * PAIR : 8, :] = inverse[2 * PAIR :]
        lo = 0 if plane < n_z // 2 else (n_z - 1) * PAIR
        aux_send[plane, 8 : 8 + PAIR, :] = slot_t[lo : lo + PAIR]
        aux_send[plane, 8 + PAIR : 8 + 2 * PAIR, :] = mixed_t[lo : lo + PAIR]
        aux_send[plane, 8 + 2 * PAIR :, :] = inverse[2 * PAIR :]
    aux_recv[z] = aux_send[z]

    def aux_copy(d):
        plane = (z + d) % n_z
        return remote(aux_send.at[plane], aux_recv.at[z], aux_s.at[d], aux_r.at[z], fs=plane * PAIR + x)

    def aux_from(plane):
        return remote(aux_send.at[plane], aux_recv.at[plane], aux_s.at[0], aux_r.at[plane], fs=me)
    for d in range(1, n_z):
        aux_copy(d).start()

    gain_mat[...] = jnp.transpose(jnp.broadcast_to(gain[...], (h_cols, d_loc)))

    def wgu_copy(d):
        e = (me + d) % n_fs
        return remote(wgu_send.at[e], wgu_recv.at[me], wgu_s.at[d], wgu_r.at[me], fs=e)

    def wgu_from(j):
        return remote(wgu_send.at[j], wgu_recv.at[j], wgu_s.at[0], wgu_r.at[j], fs=me)

    def wd_copy(d):
        e = (me + d) % n_fs
        return remote(wd_send.at[e], wd_recv.at[me], wd_s.at[d], wd_r.at[me], fs=e)

    def wd_from(j):
        return remote(wd_send.at[j], wd_recv.at[j], wd_s.at[0], wd_r.at[j], fs=me)

    def cast_gu(d, target, index):
        e = (me + d) % n_fs
        load(0, e).wait()
        load(1, e).wait()
        target[index, :, 0:h_cols] = (stage[0, e] * gain_mat[...]).astype(bf16)
        target[index, :, h_cols : 2 * h_cols] = (stage[1, e] * gain_mat[...]).astype(bf16)

    def cast_d(d, target, index):
        e = (me + d) % n_fs
        load(2, e).wait()
        target[index] = stage[2, e].astype(bf16)

    def send_gu(d):
        cast_gu(d, wgu_send, (me + d) % n_fs)
        wgu_copy(d).start()

    def send_d(d):
        e = (me + d) % n_fs
        cast_d(d, wd_send, e)
        plane = e // PAIR
        helper = jnp.where(plane == 0, 1, n_z - 2) * PAIR + e % PAIR
        by_helper = ((plane == 0) | (plane == n_z - 1)) & (plane != z) & (helper != me)

        @pl.when(by_helper)
        def _():
            remote(wd_send.at[e], wd2.at[me], wd_s.at[d], w2_r.at[me], fs=helper).start()

        @pl.when(~by_helper)
        def _():
            wd_copy(d).start()

    def span(first_d, last_d, body):
        every(last_d - first_d, lambda i: body(i + first_d))

    def picker(b, which, base=0):
        slots = aux_recv[b, pl.ds(base + which, 1), :]
        at = lax.broadcasted_iota(jnp.int32, (cap, r_rows), 0).astype(f32)
        return at == jnp.broadcast_to(slots, (cap, r_rows))

    def x_copy(b):
        return remote(xsend.at[b], rows.at[t, b, pl.ds(cap, cap)], x_s.at[b], x_r.at[b], fs=xp)

    def stage_a(s):
        b = looked_up(near, z, s)

        @pl.when(b != z)
        def _():
            ag_right(b).wait_recv()
            ag_start(b)
            aux_from(b).wait_recv()
        scale = jnp.broadcast_to(aux_recv[b, 2 * PAIR : 2 * PAIR + 1, :], (cap, r_rows))

        def compact(which):
            hit = picker(b, which)
            factor = jnp.sum(jnp.where(hit, scale, 0.0), axis=1, keepdims=True)
            taken = jnp.dot(jnp.where(hit, 1.0, 0.0).astype(bf16), blk[b], preferred_element_type=f32)
            return (taken * factor).astype(bf16)
        xsend[b] = compact(1 - x)
        x_copy(b).start()
        rows[t, b, 0:cap, :] = compact(x)

    def rc_copy(b):
        return remote(rows.at[t, b], rows.at[t, b], rc_s.at[b], rc_r.at[b], tp=tc)

    def ry_copy(b):
        return remote(rows.at[t, b], rows.at[t, b], ry_s.at[b], ry_r.at[b], tp=ty)

    def rf_copy(b):
        return remote(rows.at[ty, b], rows.at[ty, b], rf_s.at[b], rf_r.at[b], tp=tc)

    def stage_b(s):
        b = looked_up(near, z, s)
        x_copy(b).wait_recv()
        ry_copy(b).start()
        rc_copy(b).start()

    def stage_c(s):
        b = looked_up(near, z, s)
        ry_copy(b).wait_recv()
        rf_copy(b).start()

    def plane_send(plane, column, body):
        body((plane * PAIR + column + n_fs - me) % n_fs)


    def partner_sends(body):
        body((xp + n_fs - me) % n_fs)

    def named(kind, s):
        with jax.named_scope(kind + str(s)):
            {"a": stage_a, "b": stage_b, "c": stage_c}[kind](s)

    def out_copies(j):
        at = pl.ds(pl.multiple_of(j * d_loc, d_loc), d_loc)
        return [
            pltpu.make_async_copy(wgu_recv.at[j, :, pl.ds(0, h_cols)], gate_out.at[at], out_sem.at[0, j]),
            pltpu.make_async_copy(wgu_recv.at[j, :, pl.ds(h_cols, h_cols)], up_out.at[at], out_sem.at[1, j]),
            pltpu.make_async_copy(wd_recv.at[j], down_out.at[at], out_sem.at[2, j]),
        ]

    def dn_copy(j):
        q = j % per_quarter
        return remote(wd_recv.at[j], dn.at[q, t], dn_s.at[j], dn_r.at[q, t], tp=j // per_quarter)

    def dn_from(q, k):
        return remote(wd_recv.at[0], dn.at[q, k], dn_s.at[0], dn_r.at[q, k], tp=t)

    def pass_down(j):
        @pl.when(j != me)
        def _():
            wd_from(j).wait_recv()

        @pl.when(j // per_quarter == t)
        def _():
            dn[j % per_quarter, t] = wd_recv[j]

        @pl.when(j // per_quarter != t)
        def _():
            dn_copy(j).start()
        out_copies(j)[2].start()

    def pass_plane(s):
        plane = looked_up(near, z, s)
        for k in range(PAIR):
            pass_down(plane * PAIR + k)

    def wf_copy(j):
        return remote(wd2.at[j], wd_recv.at[j], wf_s.at[j], wd_r.at[j], fs=at(-1) * PAIR + x)

    def d2_copy(j):
        q = j % per_quarter
        return remote(wd2.at[j], dn2.at[q, t], d2_s.at[j], d2_r.at[q, t], tp=j // per_quarter)

    def pass_for_end(j):
        @pl.when(j == me)
        def _():
            wd2[j] = wd_send[at(-1) * PAIR + x]

        @pl.when(j != me)
        def _():
            wd_copy_at = remote(wd2.at[j], wd2.at[j], w2_s.at[0], w2_r.at[j], fs=me)
            wd_copy_at.wait_recv()

        @pl.when((j != me) & (j // PAIR != at(-1)))
        def _():
            wf_copy(j).start()

    def pass_end(j):
        @pl.when(j // per_quarter == t)
        def _():
            dn2[j % per_quarter, t] = wd2[j]

        @pl.when(j // per_quarter != t)
        def _():
            d2_copy(j).start()

    def help_end():
        for distance in (0, -1, 1, 2):
            for k in range(PAIR):
                pass_for_end(at(distance) * PAIR + k)

    def own_weights():
        cast_gu(0, wgu_recv, me)
        cast_d(0, wd_recv, me)

    def outer_own():
        own_weights()
        for k in range(PAIR):
            help_copy(k).start()

    def run(*steps):
        for step in steps:
            if isinstance(step, str):
                named(step[0], int(step[1]))
            else:
                with jax.named_scope("w"):
                    step()

    def toward(distance, column, *bodies):
        @pl.when(z < n_z // 2)
        def _():
            for each in bodies:
                plane_send(z + distance, column, each)

        @pl.when(z >= n_z // 2)
        def _():
            for each in bodies:
                plane_send(z - distance, column, each)

    def forwarded():
        @pl.when(z < n_z // 2)
        def _():
            ag_left(z + 2).wait_send()

        @pl.when(z >= n_z // 2)
        def _():
            ag_right(z - 2).wait_send()

    def partner_all():
        partner_sends(send_gu)
        partner_sends(send_d)

    def inner_second(body):
        toward(-1, x, body)
        toward(1, 1 - x, body)
        toward(-1, 1 - x, body)

    @pl.when(inner)
    def _():
        run("a0", partner_all, "b0", "a1", "a2", "c0", "a3",
            lambda: toward(2, x, send_d), lambda: toward(2, 1 - x, send_d), lambda: toward(1, x, send_gu, send_d),
            "b1", "b2", forwarded, lambda: inner_second(send_d), "c1", "b3",
            lambda: toward(2, x, send_gu), lambda: inner_second(send_gu), lambda: toward(2, 1 - x, send_gu),
            own_weights, help_end, "c2")

    def outer_second(body):
        for distance in range(1, n_z - 1):
            toward(distance, 1 - x, body)

    @pl.when(~inner)
    def _():
        run("a0", partner_all, "b0", "a1", lambda: toward(1, x, send_gu, send_d), "b1", "c0", outer_own,
            "a2", lambda: toward(3, x, send_d), lambda: toward(3, 1 - x, send_d),
            lambda: toward(2, x, send_gu, send_d), "b2", "c1", "a3", lambda: outer_second(send_d), "b3",
            lambda: toward(3, x, send_gu), lambda: outer_second(send_gu), lambda: toward(3, 1 - x, send_gu), "c2")
    with jax.named_scope("pass_own"):
        pass_plane(0)
    with jax.named_scope("c3"):
        stage_c(3)


    def hc_copy(b):
        return remote(hid.at[t, b], hid.at[t, b], hc_s.at[b], hc_r.at[b], tp=tc)

    def hy_copy(b):
        return remote(hid.at[t, b], hid.at[t, b], hy_s.at[b], hy_r.at[b], tp=ty)

    def hf_copy(b):
        return remote(hid.at[ty, b], hid.at[ty, b], hf_s.at[b], hf_r.at[b], tp=tc)

    def h2_copy(b):
        return remote(hid.at[t, b], hid2.at[t], h2_sem.at[0], h2_sem.at[1], fs=at(1) * PAIR + x)

    def h2y_copy():
        return remote(hid2.at[t], hid2.at[t], h2_sem.at[2], h2_sem.at[3], tp=ty)

    def h2c_copy():
        return remote(hid2.at[t], hid2.at[t], h2_sem.at[4], h2_sem.at[5], tp=tc)

    def h2f_copy():
        return remote(hid2.at[ty], hid2.at[ty], h2_sem.at[6], h2_sem.at[7], tp=tc)

    def rows_ready(b):
        rc_copy(b).wait_recv()
        rf_copy(b).wait_recv()

    def add_piece(j):
        lo = pl.ds(pl.multiple_of((j % per_quarter) * d_loc, d_loc), d_loc)

        def one(b):
            both[b] += jnp.dot(rows[j // per_quarter, b, :, lo], wgu_recv[j], preferred_element_type=f32)
        every(n_z, one)

    def add_plane(s):
        plane = looked_up(near, z, s)
        for k in range(PAIR):
            j = plane * PAIR + k

            @pl.when(j != me)
            def _():
                wgu_from(j).wait_recv()
            for copy in out_copies(j)[:2]:
                copy.start()
            add_piece(j)

    def stage_h(s):
        b = looked_up(far, z, s)
        gates = both[b, :, 0:h_cols]
        hid[t, b] = (gates / (1.0 + jnp.exp(-gates)) * both[b, :, h_cols:]).astype(bf16)
        apart = ~inner & (b == at(3))

        @pl.when(apart)
        def _():
            h2_copy(b).start()

        @pl.when(~apart)
        def _():
            hy_copy(b).start()
            hc_copy(b).start()
    both[...] = jnp.zeros(both.shape, f32)
    with jax.named_scope("pass"):
        span(1, n_z, pass_plane)

    @pl.when(inner)
    def _():
        every(n_fs, pass_end)
    with jax.named_scope("rows"):
        every(n_z, rows_ready)
    with jax.named_scope("gu"):
        every(n_z, add_plane)
    with jax.named_scope("h"):
        every(n_z, stage_h)

    def stage_e(s):
        b = looked_up(far, z, s)
        hy_copy(b).wait_recv()
        hf_copy(b).start()

    def wait_dn(d):
        k = (t + d) % n_tp
        for q in range(per_quarter):
            dn_from(q, k).wait_recv()
    with jax.named_scope("span_1_n_tp_wait_dn_"):
        span(1, n_tp, wait_dn)

    def y_copy(b, q):
        return remote(ysend.at[b, q], yb.at[b, q, pl.ds(cap, cap)], y_s.at[b, q], y_r.at[b, q], fs=xp)

    def stage_f(s):
        b = looked_up(far, z, s)
        hc_copy(b).wait_recv()
        hf_copy(b).wait_recv()
        units = jnp.concatenate([hid[k, b] for k in range(n_tp)], axis=1)
        for q in range(per_quarter):
            mat = jnp.concatenate([dn[q, k] for k in range(n_tp)], axis=1)
            result = lax.dot_general(units, mat, (((1,), (1,)), ((), ())), preferred_element_type=f32)
            result = result.astype(bf16)
            ysend[b, q] = result[cap:]
            y_copy(b, q).start()
            yb[b, q, 0:cap, :] = result[:cap]
    def y2_copy(q):
        return remote(ysend2.at[q], yb2.at[q, pl.ds(cap, cap)], y2_s.at[q], y2_r.at[q], fs=xp)

    def result_of(s):
        stage_e(s)
        stage_f(s)

    def end_hidden():
        h2_copy(at(2)).wait_recv()
        h2y_copy().start()
        h2c_copy().start()
        h2y_copy().wait_recv()
        h2f_copy().start()

    def wait_dn2(d):
        k = (t + d) % n_tp
        for q in range(per_quarter):
            remote(wd2.at[0], dn2.at[q, k], d2_s.at[0], d2_r.at[q, k], tp=t).wait_recv()

    def end_results():
        span(1, n_tp, wait_dn2)
        h2c_copy().wait_recv()
        h2f_copy().wait_recv()
        units = jnp.concatenate([hid2[k] for k in range(n_tp)], axis=1)
        for q in range(per_quarter):
            mat = jnp.concatenate([dn2[q, k] for k in range(n_tp)], axis=1)
            result = lax.dot_general(units, mat, (((1,), (1,)), ((), ())), preferred_element_type=f32)
            result = result.astype(bf16)
            ysend2[q] = result[cap:]
            y2_copy(q).start()
            yb2[q, 0:cap, :] = result[:cap]

    def rs_right(b, q):
        return remote(rs_send.at[b, q], rs_recv.at[b, q], rs_sr.at[b, q], rs_r.at[b, q], fs=me + PAIR)

    def rs_left(b, q):
        at = jnp.where(b == z - 1, n_z, b)
        return remote(rs_send.at[b, q], rs_recv.at[at, q], rs_sl.at[b, q], rs_r.at[at, q], fs=me - PAIR)

    def rs_from(at, q):
        return remote(rs_send.at[0, q], rs_recv.at[at, q], rs_sr.at[0, q], rs_r.at[at, q], fs=me)

    def stage_g(s, q):
        b = looked_up(far, z, s)

        helped = inner & (b == at(2))

        def share(which, base=0):
            weights = jnp.broadcast_to(aux_recv[b, pl.ds(base + PAIR + which, 1), :], (cap, r_rows))
            return jnp.where(picker(b, which, base), weights, 0.0).astype(bf16)
        spreading = jnp.concatenate([share(x), share(1 - x)], axis=0)
        y_copy(b, q).wait_recv()
        acc[...] = lax.dot_general(spreading, yb[b, q], (((0,), (0,)), ((), ())), preferred_element_type=f32)

        @pl.when(helped)
        def _():
            y2_copy(q).wait_recv()
            more = jnp.concatenate([share(x, 8), share(1 - x, 8)], axis=0)
            acc[...] += lax.dot_general(more, yb2[q], (((0,), (0,)), ((), ())), preferred_element_type=f32)

        @pl.when((((b >= z) & (z > 0)) | ((b < z) & (z < n_z - 1))) & ~helped)
        def _():
            rs_from(b, q).wait_recv()
            acc[...] += rs_recv[b, q].astype(f32)

        @pl.when((b == z) & (z < n_z - 1))
        def _():
            rs_from(n_z, q).wait_recv()
            acc[...] += rs_recv[n_z, q].astype(f32)

        @pl.when(b != z)
        def _():
            rs_send[b, q] = acc[...].astype(bf16)

        @pl.when(b > z)
        def _():
            rs_right(b, q).start()

        @pl.when(b < z)
        def _():
            rs_left(b, q).start()

        @pl.when(b == z)
        def _():
            mixed_out[:, q * d_loc : (q + 1) * d_loc] = acc[...].astype(bf16)
    def in_turn(*steps):
        for name, step, *given in steps:
            with jax.named_scope(name):
                step(*given)

    @pl.when(inner)
    def _():
        in_turn(
            ("f0", result_of, 0), ("e2", end_hidden), ("f2", end_results),
            ("g00", stage_g, 0, 0), ("f1", result_of, 1), ("g01", stage_g, 0, 1),
            ("g10", stage_g, 1, 0), ("f2", result_of, 2), ("g11", stage_g, 1, 1),
            ("f3", result_of, 3), ("g20", stage_g, 2, 0), ("g21", stage_g, 2, 1),
            ("g30", stage_g, 3, 0), ("g31", stage_g, 3, 1),
        )

    @pl.when(~inner)
    def _():
        in_turn(
            ("f1", result_of, 1), ("g10", stage_g, 1, 0), ("f2", result_of, 2), ("g11", stage_g, 1, 1),
            ("g20", stage_g, 2, 0), ("f3", result_of, 3), ("g21", stage_g, 2, 1),
            ("g30", stage_g, 3, 0), ("g31", stage_g, 3, 1),
        )

    for d in range(1, n_tp):
        ssq_copy(d).wait_send()
    for d in range(1, n_z):
        aux_copy(d).wait_send()

    def sent_w(d):
        wgu_copy(d).wait_send()
        wd_copy(d).wait_send()
    span(1, n_fs, sent_w)

    def sent_b(b):
        @pl.when(goes_right(b) & ~(inner & (b == z - 2)))
        def _():
            ag_right(b).wait_send()

        @pl.when(goes_left(b) & ~(inner & (b == z + 2)))
        def _():
            ag_left(b).wait_send()
        for copy in (x_copy, rc_copy, ry_copy, rf_copy):
            copy(b).wait_send()
        apart = ~inner & (b == at(3))

        @pl.when(apart)
        def _():
            h2_copy(b).wait_send()

        @pl.when(~apart)
        def _():
            for copy in (hc_copy, hy_copy, hf_copy):
                copy(b).wait_send()
            for q in range(per_quarter):
                y_copy(b, q).wait_send()

        @pl.when((b > z) & ~apart)
        def _():
            for q in range(per_quarter):
                rs_right(b, q).wait_send()

        @pl.when((b < z) & ~apart)
        def _():
            for q in range(per_quarter):
                rs_left(b, q).wait_send()
    every(n_z, sent_b)

    @pl.when(inner)
    def _():
        h2y_copy().wait_send()
        h2c_copy().wait_send()
        h2f_copy().wait_send()
        for q in range(per_quarter):
            y2_copy(q).wait_send()

    @pl.when(~inner)
    def _():
        for k in range(PAIR):
            help_copy(k).wait_send()

    def sent_j(j):
        @pl.when(inner & (j != me) & (j // PAIR != at(-1)))
        def _():
            wf_copy(j).wait_send()

        @pl.when(inner & (j // per_quarter != t))
        def _():
            d2_copy(j).wait_send()

        @pl.when(j // per_quarter != t)
        def _():
            dn_copy(j).wait_send()
        for copy in out_copies(j):
            copy.wait()
    every(n_fs, sent_j)


def scratch_for(dims):
    n_fs, n_tp, n_z, r_rows, feat, d_loc, h_cols, cap = dims
    f32, bf16 = jnp.float32, jnp.bfloat16
    per_quarter = feat // d_loc
    buffers = [
        ((3, n_fs, d_loc, h_cols), f32),
        ((n_fs, d_loc, 2 * h_cols), bf16),
        ((n_fs, d_loc, h_cols), bf16),
        ((n_fs, d_loc, 2 * h_cols), bf16),
        ((n_fs, d_loc, h_cols), bf16),
        ((n_z, r_rows, feat), bf16),
        ((n_tp, n_z, 2 * cap, feat), bf16),
        ((n_z, cap, feat), bf16),
        ((n_tp, n_z, 2 * cap, h_cols), bf16),
        ((per_quarter, n_tp, d_loc, h_cols), bf16),
        ((n_z, per_quarter, 2 * cap, d_loc), bf16),
        ((n_z, per_quarter, cap, d_loc), bf16),
        ((n_z, per_quarter, r_rows, d_loc), bf16),
        ((n_z + 1, per_quarter, r_rows, d_loc), bf16),
        ((r_rows, d_loc), f32),
        ((n_z, 2 * cap, 2 * h_cols), f32),
        ((n_fs, d_loc, h_cols), bf16),
        ((per_quarter, n_tp, d_loc, h_cols), bf16),
        ((n_tp, 2 * cap, h_cols), bf16),
        ((per_quarter, 2 * cap, d_loc), bf16),
        ((per_quarter, cap, d_loc), bf16),
        ((n_tp, 8, r_rows), f32),
        ((n_z, 16, r_rows), f32),
        ((n_z, 16, r_rows), f32),
        ((d_loc, h_cols), f32),
    ]
    sems = [
        (3, n_fs), (n_tp,), (n_tp,), (n_z,), (n_z,), (n_z,), (n_z,), (n_z,),
        (n_fs,), (n_fs,), (n_fs,), (n_fs,), (n_z,), (n_z,),
        (n_z,), (n_z,), (n_z,), (n_z,), (n_z,), (n_z,),
        (n_z,), (n_z,), (n_z,), (n_z,), (n_z,), (n_z,),
        (n_fs,), (per_quarter, n_tp), (n_z, per_quarter), (n_z, per_quarter),
        (n_z, per_quarter), (n_z, per_quarter), (n_z + 1, per_quarter), (3, n_fs),
        (PAIR,), (n_fs,), (n_fs,), (n_fs,), (per_quarter, n_tp), (8,), (per_quarter,), (per_quarter,),
    ]
    return buffers, sems


def dims_of(tokens, gate_master, routes):
    n_fs, n_tp = lax.axis_size("fs"), lax.axis_size("tp")
    n_experts, d_loc, h_cols = gate_master.shape
    r_rows, top_count = routes.shape
    cap = 2 * r_rows * top_count // n_experts
    return (n_fs, n_tp, n_fs // PAIR, r_rows, tokens.shape[1], d_loc, h_cols, cap)


def fits(dims, n_experts, top_count):
    n_fs, n_tp, n_z, r_rows, feat, d_loc, h_cols, cap = dims
    if n_experts != n_fs or n_fs % PAIR or n_tp != 2 * PAIR or n_z != 2 * PAIR:
        return False
    if feat % d_loc or cap % 16 or h_cols % 128 or r_rows % 128 or d_loc % 128:
        return False
    total = 4 * r_rows * feat
    for shape, kind in scratch_for(dims)[0]:
        size = jnp.dtype(kind).itemsize
        for extent in shape:
            size = size * extent
        total = total + size
    return total < VMEM_BUDGET * 9 // 10


def body(tokens, gate_master, up_master, down_master, norm_gain, routes, route_weight):
    dims = dims_of(tokens, gate_master, routes)
    if not fits(dims, gate_master.shape[0], routes.shape[1]):
        return plain_body(tokens, gate_master, up_master, down_master, norm_gain, routes, route_weight)
    n_fs, n_tp, n_z, r_rows, feat, d_loc, h_cols, cap = dims
    buffers, sems = scratch_for(dims)
    vmem, anywhere = pl.BlockSpec(memory_space=pltpu.VMEM), pl.BlockSpec(memory_space=pl.ANY)
    matrix = jax.ShapeDtypeStruct((n_fs * d_loc, h_cols), jnp.bfloat16)
    gate_out, up_out, down_out, mixed = pl.pallas_call(
        functools.partial(moe_kernel, dims),
        out_shape=(matrix, matrix, matrix, jax.ShapeDtypeStruct((r_rows, feat), jnp.bfloat16)),
        in_specs=[vmem] * 4 + [anywhere] * 3,
        out_specs=(anywhere, anywhere, anywhere, vmem),
        scratch_shapes=[pltpu.VMEM(shape, kind) for shape, kind in buffers]
        + [pltpu.SemaphoreType.DMA(shape) for shape in sems],
        compiler_params=pltpu.CompilerParams(
            collective_id=0, has_side_effects=True, vmem_limit_bytes=VMEM_BUDGET
        ),
        name="experts",
    )(tokens, norm_gain[None, :], routes.T, route_weight.T, gate_master, up_master, down_master)
    return (gate_out[None], up_out[None], down_out[None], mixed)


def solution(mesh):
    placed = (
        P("fs", "tp"),
        P(None, "fs", "tp"),
        P(None, "fs", "tp"),
        P(None, "fs", "tp"),
        P("fs"),
        P("fs", None),
        P("fs", None),
    )
    return jax.shard_map(
        body,
        mesh=mesh,
        in_specs=placed,
        out_specs=(P("fs", None, "tp"), P("fs", None, "tp"), P("fs", None, "tp"), P("fs", "tp")),
        check_vma=False,
    )
```

```python
import functools

import jax
import jax.numpy as jnp
from jax import lax
from jax.experimental import pallas as pl
from jax.experimental.pallas import tpu as pltpu
from jax.sharding import PartitionSpec as P

norm_eps = 1e-06


def half_shift(step, size):
    half = size // 2
    return [(s, s // half * half + (s % half + step) % half) for s in range(size)]


def cross_swap(size):
    return [(s, (s + size // 2) % size) for s in range(size)]


def member_shift(step, crossed, size):
    half = size // 2
    return [
        (s, (s // half + crossed) % 2 * half + (s % half + step) % half) for s in range(size)
    ]


def plain_body(tokens, gate_master, up_master, down_master, norm_gain, routes, route_weight):
    n_experts = gate_master.shape[0]
    tok_rows, top_count = routes.shape
    capacity = 2 * tok_rows * top_count // n_experts
    n_tp = lax.axis_size("tp")
    half = n_tp // 2
    width = tokens.shape[1]
    hidden_cols = gate_master.shape[2]
    me_tp = lax.axis_index("tp")
    chunks = 2 if capacity % 32 == 0 else 1
    part = capacity // chunks

    folded = norm_gain[None, :, None]
    trio = jnp.concatenate(
        [
            (gate_master * folded).astype(jnp.bfloat16),
            (up_master * folded).astype(jnp.bfloat16),
            down_master.astype(jnp.bfloat16),
        ],
        axis=2,
    )
    trio = lax.all_to_all(trio, "fs", split_axis=0, concat_axis=1, tiled=True)
    pair = trio[:, :, : 2 * hidden_cols]
    gate_out = trio[:, :, :hidden_cols]
    up_out = trio[:, :, hidden_cols : 2 * hidden_cols]
    down_out = trio[:, :, 2 * hidden_cols :]

    token_float = tokens.astype(jnp.float32)
    sumsquares = lax.psum(jnp.sum(token_float * token_float, axis=1), "tp")
    inverse = lax.rsqrt(sumsquares / (width * n_tp) + norm_eps)[:, None]
    normed = (token_float * inverse).astype(jnp.bfloat16)
    mix = route_weight / jnp.sum(route_weight, axis=1, keepdims=True)
    experts = jnp.arange(n_experts, dtype=jnp.int32)
    named = jnp.any(routes[:, :, None] == experts, axis=1)
    earlier = jnp.arange(tok_rows)[:, None] > jnp.arange(tok_rows)[None, :]
    before = jnp.dot(
        earlier.astype(jnp.bfloat16), named.astype(jnp.bfloat16), preferred_element_type=jnp.float32
    ).astype(jnp.int32)
    slots = jnp.sum(jnp.where(routes[:, :, None] == experts, before[:, None, :], 0), axis=2)
    place = (slots // part * n_experts + routes) * part + slots % part
    spots = jnp.arange(n_experts * capacity, dtype=jnp.int32)
    where_to = place[:, :, None] == spots
    onehot = jnp.any(where_to, axis=1).astype(jnp.bfloat16)
    mixing = jnp.sum(jnp.where(where_to, mix[:, :, None], 0.0), axis=1)
    mixing = mixing.astype(jnp.bfloat16)
    outgoing = lax.dot_general(
        onehot, normed, (((0,), (0,)), ((), ())), preferred_element_type=jnp.float32
    ).astype(jnp.bfloat16)
    outgoing = outgoing.reshape(chunks, n_experts, part, width)

    my_half = me_tp // half
    inside = me_tp % half
    span = half * width
    own_cols = lax.dynamic_slice_in_dim(pair[0], my_half * span, span, 0)
    partner_cols = lax.ppermute(
        lax.dynamic_slice_in_dim(pair[0], (1 - my_half) * span, span, 0), "tp", cross_swap(n_tp)
    )

    arrived = []
    for c in range(chunks):
        if c == 0:
            ready, trio = lax.optimization_barrier((outgoing[c], trio))
        else:
            ready, arrived[-1], partner_cols = lax.optimization_barrier((outgoing[c], last, partner_cols))
        last = lax.all_to_all(ready, "fs", split_axis=0, concat_axis=0, tiled=True)
        arrived.append(last)

    def in_order(cols):
        blocks = cols.reshape(half, width, cols.shape[1])
        return [
            lax.dynamic_index_in_dim(blocks, (inside + half - j) % half, 0, keepdims=False)
            for j in range(half)
        ]

    own_blocks, partner_blocks = in_order(own_cols), in_order(partner_cols)
    quarters = down_out[0].reshape(n_tp, -1, hidden_cols)
    picked = []
    for j in range(half):
        for crossed in range(2):
            target = (my_half + crossed) % 2 * half + (inside + j) % half
            piece = lax.dynamic_index_in_dim(quarters, target, 0, keepdims=False)
            if j + crossed > 0:
                piece = lax.ppermute(piece, "tp", member_shift(j, crossed, n_tp))
            picked.append(piece)
    down_mat = jnp.concatenate(picked, axis=1)

    def serve(rows):
        rows = rows.reshape(-1, width)
        pieces = [rows] + [lax.ppermute(rows, "tp", half_shift(j, n_tp)) for j in range(1, half)]

        def partial(blocks):
            total = 0.0
            for piece, block in zip(pieces, blocks):
                total = total + jnp.dot(piece, block, preferred_element_type=jnp.float32)
            return total

        swapped = lax.ppermute(partial(partner_blocks).astype(jnp.bfloat16), "tp", cross_swap(n_tp))
        both = partial(own_blocks) + swapped.astype(jnp.float32)
        hidden = (jax.nn.silu(both[:, :hidden_cols]) * both[:, hidden_cols:]).astype(jnp.bfloat16)
        two = jnp.concatenate([hidden, lax.ppermute(hidden, "tp", cross_swap(n_tp))], axis=1)
        all_hidden = [two] + [lax.ppermute(two, "tp", half_shift(j, n_tp)) for j in range(1, half)]
        result = lax.dot_general(
            jnp.concatenate(all_hidden, axis=1),
            down_mat,
            (((1,), (1,)), ((), ())),
            preferred_element_type=jnp.float32,
        )
        return result.astype(jnp.bfloat16).reshape(-1, part, width)

    returned = []
    for c in range(chunks):
        rows = arrived[c]
        if c > 0:
            rows, served = lax.optimization_barrier((rows, served))
            returned.append(lax.all_to_all(served, "fs", split_axis=0, concat_axis=0, tiled=True))
        served = serve(rows)
    returned.append(lax.all_to_all(served, "fs", split_axis=0, concat_axis=0, tiled=True))

    mixed = 0.0
    for c, back in enumerate(returned):
        flat = back.reshape(n_experts * part, width)
        chosen = mixing[:, c * n_experts * part : (c + 1) * n_experts * part]
        mixed = mixed + jnp.dot(chosen, flat, preferred_element_type=jnp.float32)
    return (gate_out, up_out, down_out, mixed.astype(jnp.bfloat16))


PAIR = 2
VMEM_BUDGET = 62 * 1024 * 1024


def near_first(n_z):
    return [sorted(range(n_z), key=lambda b: (abs(b - z), b)) for z in range(n_z)]


def far_first(n_z):
    def rank(z, b):
        return (-abs(b - z), -min(b, n_z - 1 - b), b)

    return [sorted(range(n_z), key=lambda b: rank(z, b)) for z in range(n_z)]


def looked_up(table, z, step):
    chosen = 0
    for i, row in enumerate(table):
        for s, value in enumerate(row):
            chosen = chosen + jnp.where((z == i) & (step == s), value, 0)
    return chosen


def moe_kernel(
    dims,
    tok, gain, routes, weight, gate_hbm, up_hbm, down_hbm,
    gate_out, up_out, down_out, mixed_out,
    stage, wgu_send, wd_send, wgu_recv, wd_recv, blk, rows, xsend, hid, dn, yb, ysend,
    rs_send, rs_recv, acc, both, wd2, dn2, hid2, yb2, ysend2, ssq, aux_send, aux_recv, gain_mat,
    stage_sem, ssq_s, ssq_r, aux_s, aux_r, ag_sr, ag_sl, ag_r,
    wgu_s, wgu_r, wd_s, wd_r, x_s, x_r,
    rc_s, rc_r, ry_s, ry_r, rf_s, rf_r,
    hc_s, hc_r, hy_s, hy_r, hf_s, hf_r,
    dn_s, dn_r, y_s, y_r, rs_sr, rs_sl, rs_r, out_sem,
    w2_s, w2_r, wf_s, d2_s, d2_r, h2_sem, y2_s, y2_r, mixed_sem,
):
    n_fs, n_tp, n_z, r_rows, feat, d_loc, h_cols, cap = dims
    top_count = routes.shape[0]
    f32, bf16 = jnp.float32, jnp.bfloat16
    me = lax.axis_index("fs")
    t = lax.axis_index("tp")
    z, x = me // PAIR, me % PAIR
    xp = me - x + (1 - x)
    half = n_tp // 2
    tc = (t // half) * half + (half - 1 - t % half)
    ty = (t + half) % n_tp
    near, far = near_first(n_z), far_first(n_z)
    per_quarter = feat // d_loc

    def remote(src, dst, ssem, rsem, **where):
        return pltpu.make_async_remote_copy(
            src_ref=src, dst_ref=dst, send_sem=ssem, recv_sem=rsem,
            device_id=where, device_id_type=pl.DeviceIdType.MESH,
        )

    masters = (gate_hbm, up_hbm, down_hbm)

    def load(i, e):
        return pltpu.make_async_copy(masters[i].at[e], stage.at[i, e], stage_sem.at[i, e])

    def every(count, body):
        def step(i, carry):
            body(i)
            return carry
        lax.fori_loop(0, count, step, 0)

    barrier = pltpu.get_barrier_semaphore()
    for d in range(1, n_fs):
        pl.semaphore_signal(barrier, inc=1, device_id={"fs": (me + d) % n_fs},
                            device_id_type=pl.DeviceIdType.MESH)
    for d in range(1, n_tp):
        pl.semaphore_signal(barrier, inc=1, device_id={"tp": (t + d) % n_tp},
                            device_id_type=pl.DeviceIdType.MESH)

    def start_load(d):
        for i in range(3):
            load(i, (me + d) % n_fs).start()
    every(n_fs, start_load)

    blk[z] = tok[...]

    value = tok[...].astype(f32)
    column = jnp.sum(value * value, axis=1, keepdims=True)
    spread = jnp.transpose(jnp.broadcast_to(column, (r_rows, 128)))
    ssq[t] = spread[:8]

    with jax.named_scope("bar"):
        pl.semaphore_wait(barrier, n_fs - 1 + n_tp - 1)

    def ssq_copy(d):
        peer = (t + d) % n_tp
        return remote(ssq.at[t], ssq.at[t], ssq_s.at[d], ssq_r.at[t], tp=peer)

    def ssq_from(d):
        peer = (t + n_tp - d) % n_tp
        return remote(ssq.at[peer], ssq.at[peer], ssq_s.at[d], ssq_r.at[peer], tp=peer)
    for d in range(1, n_tp):
        ssq_copy(d).start()

    def ag_right(b):
        return remote(blk.at[b], blk.at[b], ag_sr.at[b], ag_r.at[b], fs=me + PAIR)

    def ag_left(b):
        return remote(blk.at[b], blk.at[b], ag_sl.at[b], ag_r.at[b], fs=me - PAIR)

    def goes_right(b):
        return (b <= z) & (z < n_z - 1)

    def goes_left(b):
        return (b >= z) & (z > 0)

    def ag_start(b):
        @pl.when(goes_right(b))
        def _():
            ag_right(b).start()

        @pl.when(goes_left(b))
        def _():
            ag_left(b).start()
    ag_start(z)

    side = jnp.where(z < n_z // 2, 1, -1)
    inner = (z > 0) & (z < n_z - 1)

    def at(distance):
        return z + side * distance

    def help_copy(k):
        src = wd_send.at[xp] if k == 0 else wd_recv.at[me]
        column = 1 - x if k == 0 else x
        return remote(src, wd2.at[me], w2_s.at[k], w2_r.at[me], fs=at(1) * PAIR + column)

    expert = lax.broadcasted_iota(jnp.int32, (n_fs, r_rows), 0)
    picks = [jnp.broadcast_to(routes[k : k + 1, :], (n_fs, r_rows)) == expert for k in range(top_count)]
    weights = weight[...]
    mix = weights / jnp.sum(weights, axis=0, keepdims=True)
    named = jnp.zeros((n_fs, r_rows), f32)
    mixed_t = jnp.zeros((n_fs, r_rows), f32)
    for k in range(top_count):
        named = named + jnp.where(picks[k], 1.0, 0.0)
        mixed_t = mixed_t + jnp.where(picks[k], jnp.broadcast_to(mix[k : k + 1, :], (n_fs, r_rows)), 0.0)
    first = lax.broadcasted_iota(jnp.int32, (r_rows, r_rows), 0)
    second = lax.broadcasted_iota(jnp.int32, (r_rows, r_rows), 1)
    earlier = jnp.where(first < second, 1.0, 0.0).astype(bf16)
    before = jnp.dot(named.astype(bf16), earlier, preferred_element_type=f32)
    slot_t = jnp.where(named > 0.0, before, -1.0)
    with jax.named_scope("ssqwait"):
        for d in range(1, n_tp):
            ssq_from(d).wait_recv()
    total = ssq[0]
    for k in range(1, n_tp):
        total = total + ssq[k]
    inverse = lax.rsqrt(total / (feat * n_tp) + norm_eps)
    for plane in range(n_z):
        lo = plane * PAIR
        aux_send[plane, 0:PAIR, :] = slot_t[lo : lo + PAIR]
        aux_send[plane, PAIR : 2 * PAIR, :] = mixed_t[lo : lo + PAIR]
        aux_send[plane, 2 * PAIR : 8, :] = inverse[2 * PAIR :]
        lo = 0 if plane < n_z // 2 else (n_z - 1) * PAIR
        aux_send[plane, 8 : 8 + PAIR, :] = slot_t[lo : lo + PAIR]
        aux_send[plane, 8 + PAIR : 8 + 2 * PAIR, :] = mixed_t[lo : lo + PAIR]
        aux_send[plane, 8 + 2 * PAIR :, :] = inverse[2 * PAIR :]
    aux_recv[z] = aux_send[z]

    def aux_copy(d):
        plane = (z + d) % n_z
        return remote(aux_send.at[plane], aux_recv.at[z], aux_s.at[d], aux_r.at[z], fs=plane * PAIR + x)

    def aux_from(plane):
        return remote(aux_send.at[plane], aux_recv.at[plane], aux_s.at[0], aux_r.at[plane], fs=me)
    for d in range(1, n_z):
        aux_copy(d).start()

    gain_mat[...] = jnp.transpose(jnp.broadcast_to(gain[...], (h_cols, d_loc)))

    def wgu_copy(d):
        e = (me + d) % n_fs
        return remote(wgu_send.at[e], wgu_recv.at[me], wgu_s.at[d], wgu_r.at[me], fs=e)

    def wgu_from(j):
        return remote(wgu_send.at[j], wgu_recv.at[j], wgu_s.at[0], wgu_r.at[j], fs=me)

    def wd_copy(d):
        e = (me + d) % n_fs
        return remote(wd_send.at[e], wd_recv.at[me], wd_s.at[d], wd_r.at[me], fs=e)

    def wd_from(j):
        return remote(wd_send.at[j], wd_recv.at[j], wd_s.at[0], wd_r.at[j], fs=me)

    def cast_gu(d, target, index):
        e = (me + d) % n_fs
        load(0, e).wait()
        load(1, e).wait()
        target[index, :, 0:h_cols] = (stage[0, e] * gain_mat[...]).astype(bf16)
        target[index, :, h_cols : 2 * h_cols] = (stage[1, e] * gain_mat[...]).astype(bf16)

    def cast_d(d, target, index):
        e = (me + d) % n_fs
        load(2, e).wait()
        target[index] = stage[2, e].astype(bf16)

    def send_gu(d):
        cast_gu(d, wgu_send, (me + d) % n_fs)
        wgu_copy(d).start()

    def send_d(d):
        e = (me + d) % n_fs
        cast_d(d, wd_send, e)
        plane = e // PAIR
        helper = jnp.where(plane == 0, 1, n_z - 2) * PAIR + e % PAIR
        by_helper = ((plane == 0) | (plane == n_z - 1)) & (plane != z) & (helper != me)

        @pl.when(by_helper)
        def _():
            remote(wd_send.at[e], wd2.at[me], wd_s.at[d], w2_r.at[me], fs=helper).start()

        @pl.when(~by_helper)
        def _():
            wd_copy(d).start()

    def span(first_d, last_d, body):
        every(last_d - first_d, lambda i: body(i + first_d))

    def picker(b, which, base=0):
        slots = aux_recv[b, pl.ds(base + which, 1), :]
        at = lax.broadcasted_iota(jnp.int32, (cap, r_rows), 0).astype(f32)
        return at == jnp.broadcast_to(slots, (cap, r_rows))

    def x_copy(b):
        return remote(xsend.at[b], rows.at[t, b, pl.ds(cap, cap)], x_s.at[b], x_r.at[b], fs=xp)

    def ry_copy(b, part):
        some = rows.at[t, b, pl.ds(part * cap, cap)]
        return remote(some, some, ry_s.at[b, part], ry_r.at[b, part], tp=ty)

    def stage_a(s):
        b = looked_up(near, z, s)

        @pl.when(b != z)
        def _():
            ag_right(b).wait_recv()
            ag_start(b)
            aux_from(b).wait_recv()
        scale = jnp.broadcast_to(aux_recv[b, 2 * PAIR : 2 * PAIR + 1, :], (cap, r_rows))

        def compact(which):
            hit = picker(b, which)
            factor = jnp.sum(jnp.where(hit, scale, 0.0), axis=1, keepdims=True)
            taken = jnp.dot(jnp.where(hit, 1.0, 0.0).astype(bf16), blk[b], preferred_element_type=f32)
            return (taken * factor).astype(bf16)
        xsend[b] = compact(1 - x)
        x_copy(b).start()
        rows[t, b, 0:cap, :] = compact(x)
        ry_copy(b, 0).start()

    def rc_copy(b):
        return remote(rows.at[t, b], rows.at[t, b], rc_s.at[b], rc_r.at[b], tp=tc)


    def rf_copy(b):
        return remote(rows.at[ty, b], rows.at[ty, b], rf_s.at[b], rf_r.at[b], tp=tc)

    def stage_b(s):
        b = looked_up(near, z, s)
        x_copy(b).wait_recv()
        ry_copy(b, 1).start()
        rc_copy(b).start()

    def stage_c(s):
        b = looked_up(near, z, s)
        for part in range(2):
            ry_copy(b, part).wait_recv()
        rf_copy(b).start()

    def plane_send(plane, column, body):
        body((plane * PAIR + column + n_fs - me) % n_fs)


    def partner_sends(body):
        body((xp + n_fs - me) % n_fs)

    def named(kind, s):
        with jax.named_scope(kind + str(s)):
            {"a": stage_a, "b": stage_b, "c": stage_c}[kind](s)

    def out_copy(j, i):
        to = pl.ds(pl.multiple_of(j * d_loc, d_loc), d_loc)
        if i == 2:
            return pltpu.make_async_copy(wd_recv.at[j], down_out.at[to], out_sem.at[2, j])
        piece = wgu_recv.at[j, :, pl.ds(i * h_cols, h_cols)]
        return pltpu.make_async_copy(piece, (gate_out, up_out)[i].at[to], out_sem.at[i, j])

    def dn_copy(j):
        q = j % per_quarter
        return remote(wd_recv.at[j], dn.at[q, t], dn_s.at[j], dn_r.at[q, t], tp=j // per_quarter)

    def dn_from(q, k):
        return remote(wd_recv.at[0], dn.at[q, k], dn_s.at[0], dn_r.at[q, k], tp=t)

    def pass_down(j):
        @pl.when(j != me)
        def _():
            wd_from(j).wait_recv()

        @pl.when(j // per_quarter == t)
        def _():
            dn[j % per_quarter, t] = wd_recv[j]

        @pl.when(j // per_quarter != t)
        def _():
            dn_copy(j).start()
        out_copy(j, 2).start()

    def pass_plane(s):
        plane = looked_up(near, z, s)
        for k in range(PAIR):
            pass_down(plane * PAIR + k)

    def wf_copy(j):
        return remote(wd2.at[j], wd_recv.at[j], wf_s.at[j], wd_r.at[j], fs=at(-1) * PAIR + x)

    def d2_copy(j):
        q = j % per_quarter
        return remote(wd2.at[j], dn2.at[q, t], d2_s.at[j], d2_r.at[q, t], tp=j // per_quarter)

    def pass_for_end(j):
        @pl.when(j == me)
        def _():
            wd2[j] = wd_send[at(-1) * PAIR + x]

        @pl.when(j != me)
        def _():
            wd_copy_at = remote(wd2.at[j], wd2.at[j], w2_s.at[0], w2_r.at[j], fs=me)
            wd_copy_at.wait_recv()

        @pl.when((j != me) & (j // PAIR != at(-1)))
        def _():
            wf_copy(j).start()

    def pass_end(j):
        @pl.when(j // per_quarter == t)
        def _():
            dn2[j % per_quarter, t] = wd2[j]

        @pl.when(j // per_quarter != t)
        def _():
            d2_copy(j).start()

    def help_end():
        for distance in (0, -1, 1, 2):
            for k in range(PAIR):
                pass_for_end(at(distance) * PAIR + k)

    def own_weights():
        cast_gu(0, wgu_recv, me)
        cast_d(0, wd_recv, me)

    def outer_own():
        own_weights()
        for k in range(PAIR):
            help_copy(k).start()

    def run(*steps):
        for step in steps:
            if isinstance(step, str):
                named(step[0], int(step[1]))
            else:
                with jax.named_scope("w"):
                    step()

    def toward(distance, column, *bodies):
        @pl.when(z < n_z // 2)
        def _():
            for each in bodies:
                plane_send(z + distance, column, each)

        @pl.when(z >= n_z // 2)
        def _():
            for each in bodies:
                plane_send(z - distance, column, each)

    def forwarded():
        @pl.when(z < n_z // 2)
        def _():
            ag_left(z + 2).wait_send()

        @pl.when(z >= n_z // 2)
        def _():
            ag_right(z - 2).wait_send()

    def partner_all():
        partner_sends(send_gu)
        partner_sends(send_d)

    def inner_second(body):
        toward(-1, x, body)
        toward(1, 1 - x, body)
        toward(-1, 1 - x, body)

    @pl.when(inner)
    def _():
        run("a0", partner_all, "b0", "a1", "a2", "c0", "a3",
            lambda: toward(2, x, send_d), lambda: toward(2, 1 - x, send_d), lambda: toward(1, x, send_gu, send_d),
            "b1", "b2", forwarded, lambda: inner_second(send_d), "c1", "b3",
            lambda: toward(2, x, send_gu), lambda: inner_second(send_gu), lambda: toward(2, 1 - x, send_gu),
            own_weights, help_end, "c2")

    def outer_second(body):
        for distance in range(1, n_z - 1):
            toward(distance, 1 - x, body)

    @pl.when(~inner)
    def _():
        run("a0", partner_all, "b0", "a1", lambda: toward(1, x, send_gu, send_d), "b1", "c0", outer_own,
            "a2", lambda: toward(3, x, send_d), lambda: toward(3, 1 - x, send_d),
            lambda: toward(2, x, send_gu, send_d), "b2", "c1", "a3", lambda: outer_second(send_d), "b3",
            lambda: toward(3, x, send_gu), lambda: outer_second(send_gu), lambda: toward(3, 1 - x, send_gu), "c2")
    with jax.named_scope("pass_own"):
        pass_plane(0)
    with jax.named_scope("c3"):
        stage_c(3)


    def hc_copy(b):
        return remote(hid.at[t, b], hid.at[t, b], hc_s.at[b], hc_r.at[b], tp=tc)

    def hy_copy(b):
        return remote(hid.at[t, b], hid.at[t, b], hy_s.at[b], hy_r.at[b], tp=ty)

    def hf_copy(b):
        return remote(hid.at[ty, b], hid.at[ty, b], hf_s.at[b], hf_r.at[b], tp=tc)

    def h2_copy(b):
        return remote(hid.at[t, b], hid2.at[t], h2_sem.at[0], h2_sem.at[1], fs=at(1) * PAIR + x)

    def h2y_copy():
        return remote(hid2.at[t], hid2.at[t], h2_sem.at[2], h2_sem.at[3], tp=ty)

    def h2c_copy():
        return remote(hid2.at[t], hid2.at[t], h2_sem.at[4], h2_sem.at[5], tp=tc)

    def h2f_copy():
        return remote(hid2.at[ty], hid2.at[ty], h2_sem.at[6], h2_sem.at[7], tp=tc)

    def rows_ready(b):
        rc_copy(b).wait_recv()
        rf_copy(b).wait_recv()

    def add_piece(j):
        lo = pl.ds(pl.multiple_of((j % per_quarter) * d_loc, d_loc), d_loc)

        def one(b):
            both[b] += jnp.dot(rows[j // per_quarter, b, :, lo], wgu_recv[j], preferred_element_type=f32)
        every(n_z, one)

    def add_plane(s):
        plane = looked_up(near, z, s)
        for k in range(PAIR):
            j = plane * PAIR + k

            @pl.when(j != me)
            def _():
                wgu_from(j).wait_recv()
            for i in range(2):
                out_copy(j, i).start()
            add_piece(j)

    def stage_h(s):
        b = looked_up(far, z, s)
        gates = both[b, :, 0:h_cols]
        hid[t, b] = (gates / (1.0 + jnp.exp(-gates)) * both[b, :, h_cols:]).astype(bf16)
        apart = ~inner & (b == at(3))

        @pl.when(apart)
        def _():
            h2_copy(b).start()

        @pl.when(~apart)
        def _():
            hy_copy(b).start()
            hc_copy(b).start()
    both[...] = jnp.zeros(both.shape, f32)
    with jax.named_scope("pass"):
        span(1, n_z, pass_plane)

    @pl.when(inner)
    def _():
        every(n_fs, pass_end)
    with jax.named_scope("rows"):
        every(n_z, rows_ready)
    with jax.named_scope("gu"):
        every(n_z, add_plane)
    def stage_e(s):
        b = looked_up(far, z, s)
        hy_copy(b).wait_recv()
        hf_copy(b).start()

    def wait_dn(d):
        k = (t + d) % n_tp
        for q in range(per_quarter):
            dn_from(q, k).wait_recv()
    with jax.named_scope("span_1_n_tp_wait_dn_"):
        span(1, n_tp, wait_dn)

    def y_copy(b, q):
        return remote(ysend.at[b, q], yb.at[b, q, pl.ds(cap, cap)], y_s.at[b, q], y_r.at[b, q], fs=xp)

    def stage_f(s, q):
        b = looked_up(far, z, s)
        if q == 0:
            stage_e(s)
            hc_copy(b).wait_recv()
            hf_copy(b).wait_recv()
        units = jnp.concatenate([hid[k, b] for k in range(n_tp)], axis=1)
        mat = jnp.concatenate([dn[q, k] for k in range(n_tp)], axis=1)
        result = lax.dot_general(units, mat, (((1,), (1,)), ((), ())), preferred_element_type=f32)
        result = result.astype(bf16)
        ysend[b, q] = result[cap:]
        y_copy(b, q).start()
        yb[b, q, 0:cap, :] = result[:cap]

    def y2_copy(q):
        return remote(ysend2.at[q], yb2.at[q, pl.ds(cap, cap)], y2_s.at[q], y2_r.at[q], fs=xp)

    def end_hidden():
        h2_copy(at(2)).wait_recv()
        h2y_copy().start()
        h2c_copy().start()
        h2y_copy().wait_recv()
        h2f_copy().start()

    def wait_dn2(d):
        k = (t + d) % n_tp
        for q in range(per_quarter):
            remote(wd2.at[0], dn2.at[q, k], d2_s.at[0], d2_r.at[q, k], tp=t).wait_recv()

    def end_results(q):
        if q == 0:
            span(1, n_tp, wait_dn2)
            h2c_copy().wait_recv()
            h2f_copy().wait_recv()
        units = jnp.concatenate([hid2[k] for k in range(n_tp)], axis=1)
        mat = jnp.concatenate([dn2[q, k] for k in range(n_tp)], axis=1)
        result = lax.dot_general(units, mat, (((1,), (1,)), ((), ())), preferred_element_type=f32)
        result = result.astype(bf16)
        ysend2[q] = result[cap:]
        y2_copy(q).start()
        yb2[q, 0:cap, :] = result[:cap]

    def rs_right(b, q):
        return remote(rs_send.at[b, q], rs_recv.at[b, q], rs_sr.at[b, q], rs_r.at[b, q], fs=me + PAIR)

    def rs_left(b, q):
        at = jnp.where(b == z - 1, n_z, b)
        return remote(rs_send.at[b, q], rs_recv.at[at, q], rs_sl.at[b, q], rs_r.at[at, q], fs=me - PAIR)

    def rs_from(at, q):
        return remote(rs_send.at[0, q], rs_recv.at[at, q], rs_sr.at[0, q], rs_r.at[at, q], fs=me)

    def mixed_copy(q):
        lanes = pl.ds(q * d_loc, d_loc)
        return pltpu.make_async_copy(rs_send.at[z, q], mixed_out.at[:, lanes], mixed_sem.at[q])

    def stage_g(s, q):
        b = looked_up(far, z, s)

        helped = inner & (b == at(2))

        def share(which, base=0):
            weights = jnp.broadcast_to(aux_recv[b, pl.ds(base + PAIR + which, 1), :], (cap, r_rows))
            return jnp.where(picker(b, which, base), weights, 0.0).astype(bf16)
        spreading = jnp.concatenate([share(x), share(1 - x)], axis=0)
        y_copy(b, q).wait_recv()
        acc[...] = lax.dot_general(spreading, yb[b, q], (((0,), (0,)), ((), ())), preferred_element_type=f32)

        @pl.when(helped)
        def _():
            y2_copy(q).wait_recv()
            more = jnp.concatenate([share(x, 8), share(1 - x, 8)], axis=0)
            acc[...] += lax.dot_general(more, yb2[q], (((0,), (0,)), ((), ())), preferred_element_type=f32)

        @pl.when((((b >= z) & (z > 0)) | ((b < z) & (z < n_z - 1))) & ~helped)
        def _():
            rs_from(b, q).wait_recv()
            acc[...] += rs_recv[b, q].astype(f32)

        @pl.when((b == z) & (z < n_z - 1))
        def _():
            rs_from(n_z, q).wait_recv()
            acc[...] += rs_recv[n_z, q].astype(f32)

        @pl.when(b != z)
        def _():
            rs_send[b, q] = acc[...].astype(bf16)

        @pl.when(b > z)
        def _():
            rs_right(b, q).start()

        @pl.when(b < z)
        def _():
            rs_left(b, q).start()

        @pl.when(b == z)
        def _():
            rs_send[b, q] = acc[...].astype(bf16)
            mixed_copy(q).start()
    def settle():
        for d in range(1, n_tp):
            ssq_copy(d).wait_send()
        for d in range(1, n_z):
            aux_copy(d).wait_send()

        def sent_w(d):
            wgu_copy(d).wait_send()
            wd_copy(d).wait_send()
        span(1, n_fs, sent_w)

        def sent_b(b):
            @pl.when(goes_right(b) & ~(inner & (b == z - 2)))
            def _():
                ag_right(b).wait_send()

            @pl.when(goes_left(b) & ~(inner & (b == z + 2)))
            def _():
                ag_left(b).wait_send()
            for copy in (x_copy, rc_copy, rf_copy):
                copy(b).wait_send()
            for part in range(2):
                ry_copy(b, part).wait_send()
            apart = ~inner & (b == at(3))

            @pl.when(apart)
            def _():
                h2_copy(b).wait_send()

            @pl.when(~apart)
            def _():
                for copy in (hc_copy, hy_copy, hf_copy):
                    copy(b).wait_send()
        every(n_z, sent_b)

        @pl.when(inner)
        def _():
            h2y_copy().wait_send()
            h2c_copy().wait_send()
            h2f_copy().wait_send()

        @pl.when(~inner)
        def _():
            for k in range(PAIR):
                help_copy(k).wait_send()

        def sent_j(j):
            @pl.when(inner & (j != me) & (j // PAIR != at(-1)))
            def _():
                wf_copy(j).wait_send()

            @pl.when(inner & (j // per_quarter != t))
            def _():
                d2_copy(j).wait_send()

            @pl.when(j // per_quarter != t)
            def _():
                dn_copy(j).wait_send()
            for i in range(3):
                out_copy(j, i).wait()
        every(n_fs, sent_j)

    def in_turn(*steps):
        for name, step, *given in steps:
            with jax.named_scope(name):
                step(*given)

    @pl.when(inner)
    def _():
        in_turn(
            ("h", every, n_z, stage_h), ("f00", stage_f, 0, 0), ("f01", stage_f, 0, 1),
            ("e2", end_hidden), ("z0", end_results, 0), ("z1", end_results, 1), ("g00", stage_g, 0, 0),
            ("f10", stage_f, 1, 0), ("f11", stage_f, 1, 1), ("g01", stage_g, 0, 1), ("g10", stage_g, 1, 0),
            ("f20", stage_f, 2, 0), ("f21", stage_f, 2, 1), ("g11", stage_g, 1, 1), ("f30", stage_f, 3, 0),
            ("f31", stage_f, 3, 1), ("g20", stage_g, 2, 0), ("g21", stage_g, 2, 1), ("settle", settle),
            ("g30", stage_g, 3, 0), ("g31", stage_g, 3, 1),
        )

    @pl.when(~inner)
    def _():
        in_turn(
            ("h", every, n_z, stage_h), ("f10", stage_f, 1, 0), ("f11", stage_f, 1, 1), ("g10", stage_g, 1, 0),
            ("f20", stage_f, 2, 0), ("f21", stage_f, 2, 1), ("g11", stage_g, 1, 1), ("g20", stage_g, 2, 0),
            ("f30", stage_f, 3, 0), ("f31", stage_f, 3, 1), ("g21", stage_g, 2, 1), ("settle", settle),
            ("g30", stage_g, 3, 0), ("g31", stage_g, 3, 1),
        )

    def last_sent(b):
        apart = ~inner & (b == at(3))

        @pl.when(~apart)
        def _():
            for q in range(per_quarter):
                y_copy(b, q).wait_send()

        @pl.when((b > z) & ~apart)
        def _():
            for q in range(per_quarter):
                rs_right(b, q).wait_send()

        @pl.when((b < z) & ~apart)
        def _():
            for q in range(per_quarter):
                rs_left(b, q).wait_send()
    every(n_z, last_sent)
    for q in range(per_quarter):
        mixed_copy(q).wait()

        @pl.when(inner)
        def _():
            y2_copy(q).wait_send()


def publish_kernel(count, *refs):
    sources, targets = refs[:count], refs[count : 2 * count]
    buffers, (come, go) = refs[2 * count : 3 * count], refs[3 * count :]

    def inward(i):
        return pltpu.make_async_copy(sources[i], buffers[i], come.at[i])

    def outward(i):
        return pltpu.make_async_copy(buffers[i], targets[i], go.at[i])
    for i in range(count):
        inward(i).start()
    for i in range(count):
        inward(i).wait()
        outward(i).start()
    for i in range(count):
        outward(i).wait()


def publish(*arrays):
    anywhere = pl.BlockSpec(memory_space=pl.ANY)
    count = len(arrays)
    return pl.pallas_call(
        functools.partial(publish_kernel, count),
        out_shape=tuple(jax.ShapeDtypeStruct(a.shape, a.dtype) for a in arrays),
        in_specs=[anywhere] * count,
        out_specs=(anywhere,) * count,
        scratch_shapes=[pltpu.VMEM(a.shape, a.dtype) for a in arrays]
        + [pltpu.SemaphoreType.DMA((count,))] * 2,
        name="publish",
    )(*arrays)


def scratch_for(dims):
    n_fs, n_tp, n_z, r_rows, feat, d_loc, h_cols, cap = dims
    f32, bf16 = jnp.float32, jnp.bfloat16
    per_quarter = feat // d_loc
    buffers = [
        ((3, n_fs, d_loc, h_cols), f32),
        ((n_fs, d_loc, 2 * h_cols), bf16),
        ((n_fs, d_loc, h_cols), bf16),
        ((n_fs, d_loc, 2 * h_cols), bf16),
        ((n_fs, d_loc, h_cols), bf16),
        ((n_z, r_rows, feat), bf16),
        ((n_tp, n_z, 2 * cap, feat), bf16),
        ((n_z, cap, feat), bf16),
        ((n_tp, n_z, 2 * cap, h_cols), bf16),
        ((per_quarter, n_tp, d_loc, h_cols), bf16),
        ((n_z, per_quarter, 2 * cap, d_loc), bf16),
        ((n_z, per_quarter, cap, d_loc), bf16),
        ((n_z, per_quarter, r_rows, d_loc), bf16),
        ((n_z + 1, per_quarter, r_rows, d_loc), bf16),
        ((r_rows, d_loc), f32),
        ((n_z, 2 * cap, 2 * h_cols), f32),
        ((n_fs, d_loc, h_cols), bf16),
        ((per_quarter, n_tp, d_loc, h_cols), bf16),
        ((n_tp, 2 * cap, h_cols), bf16),
        ((per_quarter, 2 * cap, d_loc), bf16),
        ((per_quarter, cap, d_loc), bf16),
        ((n_tp, 8, r_rows), f32),
        ((n_z, 16, r_rows), f32),
        ((n_z, 16, r_rows), f32),
        ((d_loc, h_cols), f32),
    ]
    sems = [
        (3, n_fs), (n_tp,), (n_tp,), (n_z,), (n_z,), (n_z,), (n_z,), (n_z,),
        (n_fs,), (n_fs,), (n_fs,), (n_fs,), (n_z,), (n_z,),
        (n_z,), (n_z,), (n_z, 2), (n_z, 2), (n_z,), (n_z,),
        (n_z,), (n_z,), (n_z,), (n_z,), (n_z,), (n_z,),
        (n_fs,), (per_quarter, n_tp), (n_z, per_quarter), (n_z, per_quarter),
        (n_z, per_quarter), (n_z, per_quarter), (n_z + 1, per_quarter), (3, n_fs),
        (PAIR,), (n_fs,), (n_fs,), (n_fs,), (per_quarter, n_tp), (8,), (per_quarter,), (per_quarter,), (per_quarter,),
    ]
    return buffers, sems


def dims_of(tokens, gate_master, routes):
    n_fs, n_tp = lax.axis_size("fs"), lax.axis_size("tp")
    n_experts, d_loc, h_cols = gate_master.shape
    r_rows, top_count = routes.shape
    cap = 2 * r_rows * top_count // n_experts
    return (n_fs, n_tp, n_fs // PAIR, r_rows, tokens.shape[1], d_loc, h_cols, cap)


def fits(dims, n_experts, top_count):
    n_fs, n_tp, n_z, r_rows, feat, d_loc, h_cols, cap = dims
    if n_experts != n_fs or n_fs % PAIR or n_tp != 2 * PAIR or n_z != 2 * PAIR:
        return False
    if feat % d_loc or cap % 16 or h_cols % 128 or r_rows % 128 or d_loc % 128:
        return False
    total = 4 * r_rows * feat
    for shape, kind in scratch_for(dims)[0]:
        size = jnp.dtype(kind).itemsize
        for extent in shape:
            size = size * extent
        total = total + size
    return total < VMEM_BUDGET * 9 // 10


def body(tokens, gate_master, up_master, down_master, norm_gain, routes, route_weight):
    dims = dims_of(tokens, gate_master, routes)
    if not fits(dims, gate_master.shape[0], routes.shape[1]):
        return plain_body(tokens, gate_master, up_master, down_master, norm_gain, routes, route_weight)
    n_fs, n_tp, n_z, r_rows, feat, d_loc, h_cols, cap = dims
    buffers, sems = scratch_for(dims)
    vmem, anywhere = pl.BlockSpec(memory_space=pltpu.VMEM), pl.BlockSpec(memory_space=pl.ANY)
    matrix = jax.ShapeDtypeStruct((n_fs * d_loc, h_cols), jnp.bfloat16)
    gate_out, up_out, down_out, mixed = pl.pallas_call(
        functools.partial(moe_kernel, dims),
        out_shape=(matrix, matrix, matrix, jax.ShapeDtypeStruct((r_rows, feat), jnp.bfloat16)),
        in_specs=[vmem] * 4 + [anywhere] * 3,
        out_specs=(anywhere, anywhere, anywhere, anywhere),
        scratch_shapes=[pltpu.VMEM(shape, kind) for shape, kind in buffers]
        + [pltpu.SemaphoreType.DMA(shape) for shape in sems],
        compiler_params=pltpu.CompilerParams(
            collective_id=0, has_side_effects=True, vmem_limit_bytes=VMEM_BUDGET
        ),
        name="experts",
    )(tokens, norm_gain[None, :], routes.T, route_weight.T, gate_master, up_master, down_master)
    gate_out, up_out, down_out, mixed = publish(gate_out, up_out, down_out, mixed)
    return (gate_out[None], up_out[None], down_out[None], mixed)


def solution(mesh):
    placed = (
        P("fs", "tp"),
        P(None, "fs", "tp"),
        P(None, "fs", "tp"),
        P(None, "fs", "tp"),
        P("fs"),
        P("fs", None),
        P("fs", None),
    )
    return jax.shard_map(
        body,
        mesh=mesh,
        in_specs=placed,
        out_specs=(P("fs", None, "tp"), P("fs", None, "tp"), P("fs", None, "tp"), P("fs", "tp")),
        check_vma=False,
    )
```
